512 devices in a mesh: sp: 32 (over z, core), tp: 16 (over y, x).
Axes of the slice: x: 4, y: 4, z: 16, core: 2. Of those that a mesh axis runs over, the one named last changes fastest.
Arguments:
- residual: bfloat16 [6144, 2048], P('sp'), may hold values from -6 to 6
- query_in: bfloat16 [6144, 2048], P('sp', 'tp'), may hold values from -6 to 6
- value_in: bfloat16 [6144, 2048], P('sp', 'tp'), may hold values from -6 to 6
- forget_fwd: bfloat16 [6144, 2048], P('sp', 'tp'), may hold values from -4.5 to 4.5
- forget_bwd: bfloat16 [6144, 2048], P('sp', 'tp'), may hold values from -4.5 to 4.5
- jumps: float32 [16, 6144], P('tp', 'sp'), may hold values from -2.8 to 0
- gate_gap: float32 [2, 2048], P(None, 'tp'), may hold values from 0 to 0.1
- out_gate: bfloat16 [6144, 2048], P('sp', 'tp'), may hold values from -6 to 6
- head_gain: float32 [2048], P('tp'), may hold values from 0.1 to 1.9
- out_weight: bfloat16 [2048, 2048], P('tp'), may hold values from -0.25 to 0.25
- norm_gain: float32 [2048], replicated, may hold values from 0.1 to 1.9
- route_ids: int32 [6144, 4], P('sp'), may hold values from 0 to 31, all different within a row; in each aligned block of 192 rows (0 to 191, 192 to 383, ...) at most 36 rows name the same one
- route_weights: float32 [6144, 4], P('sp'), may hold values from 0.05 to 0.5
- w_gate: bfloat16 [32, 2048, 4096], P('sp', None, 'tp'), may hold values from -0.375 to 0.375
- w_up: bfloat16 [32, 2048, 4096], P('sp', None, 'tp'), may hold values from -0.375 to 0.375
- w_down: bfloat16 [32, 4096, 2048], P('sp', None, 'tp'), may hold values from -0.09375 to 0.09375
Outputs:
- mixed: bfloat16 [6144, 2048], P('sp', 'tp')
The draws below stay inside these ranges and needn't reach their ends.
Inputs may be any that keep to these rules, and one draw needn't show every extreme that they name: `route_ids`: in each aligned block of 192 rows each expert is named by at most 36 rows, and by exactly 36 in some block; each row names 4 different experts.
All inputs are finite; a program needn't handle non-finite values.
Results may differ from the reference program's by a relative error of at most 0.024.
Values may be sent and summed in bfloat16 or wider, within the bound.
No kernel may reach another device: no remote copies, remote signals or barrier semaphores. Data moves between devices by JAX's collectives and lax.ppermute only.
A program may use at most 64 MiB of HBM per device.

```python
import math
import jax
import jax.numpy as jnp
import numpy as np
from jax import lax

HEADS = 16
HEAD_DIM = 128
D = 2048
FF = 4096
EXPERTS = 32
TOP = 4
TOK_SP = 192
TOKENS = 6144
CAP = 36
N_SP = 32
N_TP = 16


def draw_gate_gap(key, part):
    head_key, fast_key, slow_key = jax.random.split(jax.random.fold_in(key, 11), 3)
    fast_share = 0.5
    fast_heads = jax.random.uniform(head_key, (2, HEADS, 1), jnp.float32) < fast_share
    fast_gap = jax.random.uniform(fast_key, (2, HEADS, HEAD_DIM), jnp.float32, math.log(0.03), math.log(0.1))
    slow_gap = jax.random.uniform(slow_key, (2, HEADS, HEAD_DIM), jnp.float32, math.log(0.2), 0.0)
    gap_values = jnp.where(fast_heads, jnp.exp(fast_gap), jnp.exp(slow_gap) / TOKENS)
    return gap_values.reshape(2, D).astype(jnp.float32)


def forget_values(key):
    noise_key, level_key = jax.random.split(key)
    noise = jnp.clip(jax.random.normal(noise_key, (TOKENS, D), jnp.float32), -3.0, 3.0)
    levels = jax.random.uniform(level_key, (TOKENS // TOK_SP, 1, HEADS, 1), jnp.float32, -1.5, 1.5)
    shifted = noise.reshape(TOKENS // TOK_SP, TOK_SP, HEADS, HEAD_DIM) + levels
    return shifted.reshape(TOKENS, D).astype(jnp.bfloat16)


def draw_forget_fwd(key, part):
    return forget_values(jax.random.fold_in(key, 21))


def draw_forget_bwd(key, part):
    return forget_values(jax.random.fold_in(key, 22))


def draw_jumps(key, part):
    spot_key, size_key = jax.random.split(jax.random.fold_in(key, 31))
    spots = jax.random.randint(spot_key, (HEADS, 4), 0, TOKENS)
    sizes = jax.random.uniform(size_key, (HEADS, 4), jnp.float32, math.log(0.5), math.log(0.8))
    hits = jnp.arange(TOKENS, dtype=jnp.int32)[None, :, None] == spots[:, None, :]
    return jnp.sum(jnp.where(hits, sizes[:, None, :], 0.0), axis=2).astype(jnp.float32)


def block_scale(stream_key, shape, shards, smallest, high):
    loudness = 1.0
    for dim, blocks in shards:
        heights = jax.random.uniform(jax.random.fold_in(jax.random.fold_in(stream_key, 6), dim), (blocks,), jnp.float32, smallest / len(shards), high / len(shards))
        loudness = loudness * jnp.repeat(jnp.exp(heights), shape[dim] // blocks).reshape((-1,) + (1,) * (len(shape) - 1 - dim))
    return loudness


def shared_out(key, own, number, rows, number_of, top, limit, slope):
    ranking = jax.random.permutation(key, number_of)
    packed, common = shares(number_of, rows * top, limit, slope, True), shares(number_of, rows * top, limit, slope, False)
    places = jnp.arange(number_of)

    def named(tallies, turn):
        used = int((tallies > 0).sum())
        fixed = max(1, used // 4)
        moved = fixed + (places - fixed + turn * (used - fixed)) % max(1, number_of - fixed)
        return jnp.zeros((number_of,), jnp.int32).at[ranking[jnp.where(places < fixed, places, moved)]].set(jnp.asarray(tallies, jnp.int32))

    tallies = jnp.where(number % 4 == 0, named(packed, number // 4), named(common, number - number // 4 - 1))
    mixed = jax.random.permutation(jax.random.fold_in(own, 3), number_of)
    source_of, taker = mixed[0:number_of // 2 * 2:2], mixed[1:number_of // 2 * 2:2]
    slack = jnp.minimum(tallies[source_of] - 1, limit - tallies[taker]) // 2
    slack = jnp.where((source_of == ranking[0]) | (taker == ranking[0]) | (tallies[taker] == 0), 0, jnp.maximum(slack, 0))
    moved = jax.random.randint(jax.random.fold_in(own, 4), (number_of // 2,), 0, 1 << 20) % (slack + 1)
    tallies = tallies.at[source_of].add(-moved).at[taker].add(moved)
    labels = jnp.searchsorted(jnp.cumsum(tallies), jnp.arange(rows * top), side="right").astype(jnp.int32)
    grid = labels.reshape(top, rows).T
    grid = grid[jax.random.permutation(jax.random.fold_in(own, 1), rows)]
    turn = jax.random.randint(jax.random.fold_in(own, 2), (rows, 1), 0, top)
    return jnp.take_along_axis(grid, (jnp.arange(top)[None, :] + turn) % top, axis=1)


def shares(number_of, total, reach, lean, full):
    weights = [(1 << 20) // math.isqrt(grade ** lean) + 1 for grade in range(1, number_of + 1)]
    largest = reach if full else min(reach, max(-(-total // number_of), total * weights[0] // sum(weights)))
    least = 1 if total - largest >= number_of - 1 else 0
    counts, surplus = [largest] + [least] * (number_of - 1), total - largest - least * (number_of - 1)
    while surplus > 0:
        movable = [i for i in range(1, number_of) if counts[i] < largest] or [i for i in range(1, number_of) if counts[i] < reach]
        pool, left = sum([weights[i] for i in movable]), surplus
        for i in movable:
            extra = min(reach - counts[i], max(1, left * weights[i] // pool), surplus)
            counts[i] = counts[i] + extra
            surplus = surplus - extra
    return np.array(counts)


def scatter_about(stream_key, shape, scale, bound, pieces=(), held_as=jnp.bfloat16):
    entries = scale * jax.random.normal(stream_key, shape, jnp.float32)
    if pieces:
        entries = entries * block_scale(stream_key, shape, pieces, -0.22, 0.18)
    return jnp.clip(entries, -bound, bound).astype(held_as)


def setup_inputs(seed: int = 0) -> dict:
    streams_of = jax.random.split(jax.random.key(seed), 17)
    residual = scatter_about(streams_of[0], (TOKENS, D), 1.0, 6.0, ((0, 32),))
    query_in = scatter_about(streams_of[1], (TOKENS, D), 1.0, 6.0, ((0, 32), (1, 16)))
    value_in = scatter_about(streams_of[2], (TOKENS, D), 1.0, 6.0, ((0, 32), (1, 16)))
    forget_fwd = draw_forget_fwd(jax.random.fold_in(streams_of[16], 71), 0)
    forget_bwd = draw_forget_bwd(jax.random.fold_in(streams_of[16], 71), 0)
    jumps = draw_jumps(jax.random.fold_in(streams_of[16], 71), 0)
    gate_gap = draw_gate_gap(jax.random.fold_in(streams_of[16], 71), 0)
    out_gate = scatter_about(streams_of[7], (TOKENS, D), 1.0, 6.0, ((0, 32), (1, 16)))
    head_gain = jnp.clip(1.0 + 0.18 * jax.random.normal(streams_of[8], (D,), jnp.float32), 0.1, 1.9)
    out_weight = scatter_about(streams_of[9], (D, D), (D // 4) ** -0.5, 0.25, ((0, 16),))
    norm_gain = jnp.clip(1.0 + 0.18 * jax.random.normal(streams_of[10], (D,), jnp.float32), 0.1, 1.9)
    route_ids_keys = jax.random.split(jax.random.fold_in(streams_of[11], 1), TOKENS // TOK_SP)
    route_ids_turns = jax.random.permutation(jax.random.fold_in(streams_of[11], 3), TOKENS // TOK_SP)
    route_ids = jax.vmap(lambda own, number: shared_out(jax.random.fold_in(streams_of[11], 2), own, number, TOK_SP, EXPERTS, TOP, CAP, 1))(route_ids_keys, route_ids_turns).reshape((TOKENS, TOP))
    route_weights = jnp.clip(jnp.exp(math.log(0.5) - 2.3025851 * jax.random.uniform(streams_of[12], (TOKENS, TOP), jnp.float32) ** block_scale(streams_of[12], (TOKENS, TOP), ((0, 32),), -0.2, 0.2)), 0.05, 0.5)
    w_gate = scatter_about(streams_of[13], (EXPERTS, D, FF), (D // 8) ** -0.5, 0.375, ((0, 32), (2, 16)))
    w_up = scatter_about(streams_of[14], (EXPERTS, D, FF), (D // 8) ** -0.5, 0.375, ((0, 32), (2, 16)))
    w_down = scatter_about(streams_of[15], (EXPERTS, FF, D), FF ** -0.5, 0.09375, ((0, 32), (2, 16)))
    return dict(residual=residual, query_in=query_in, value_in=value_in, forget_fwd=forget_fwd, forget_bwd=forget_bwd, jumps=jumps, gate_gap=gate_gap, out_gate=out_gate, head_gain=head_gain, out_weight=out_weight, norm_gain=norm_gain, route_ids=route_ids, route_weights=route_weights, w_gate=w_gate, w_up=w_up, w_down=w_down)


highest_precision = lax.Precision.HIGHEST
eps_norm = 1e-06
limit_value = 7.0
alpha_value = 1.702

def recurrence(queries, keys_in, values, logs):

    def advance(current_state, step_items):
        current_query, key_now, value_now, log_now = step_items
        current_state = current_state * jnp.exp(log_now)[:, :, None] + key_now[:, :, None] * value_now[:, None, :]
        return (current_state, jnp.einsum('ob,obs->os', current_query, current_state, precision=highest_precision))
    zero_state = jnp.zeros((queries.shape[1], queries.shape[2], values.shape[2]), jnp.float32)
    unused, outputs = lax.scan(advance, zero_state, (queries, keys_in, values, logs))
    return outputs

def reference(residual, query_in, value_in, forget_fwd, forget_bwd, jumps, gate_gap, out_gate, head_gain, out_weight, norm_gain, route_ids, route_weights, w_gate, w_up, w_down):
    tokens, width = query_in.shape
    head_count = jumps.shape[0]
    head_width = width // head_count

    def by_head(array):
        return array.astype(jnp.float32).reshape(tokens, head_count, head_width)
    queries = jax.nn.silu(by_head(query_in))
    values = by_head(value_in)
    jump_rows = jnp.transpose(jumps)[:, :, None]

    def gate_terms(forget_in, gap):
        key_share = gap.reshape(head_count, head_width) * jax.nn.sigmoid(-by_head(forget_in))
        return (key_share, jnp.log1p(-key_share) + jump_rows)
    keys_fwd, logs_fwd = gate_terms(forget_fwd, gate_gap[0])
    keys_bwd, logs_bwd = gate_terms(forget_bwd, gate_gap[1])
    forward_out = recurrence(queries, keys_fwd, values, logs_fwd)
    backward_out = jnp.flip(recurrence(jnp.flip(queries, 0), jnp.flip(keys_bwd, 0), jnp.flip(values, 0), jnp.flip(logs_bwd, 0)), 0)
    mixed_heads = forward_out + backward_out
    mean_square = lax.optimization_barrier(jnp.mean(mixed_heads * mixed_heads, axis=-1, keepdims=True))
    normed = (mixed_heads * lax.rsqrt(mean_square + eps_norm)).reshape(tokens, width)
    gated = (normed * head_gain * jax.nn.silu(out_gate.astype(jnp.float32))).astype(jnp.bfloat16)
    group_width = width // N_TP
    gated_groups = jnp.transpose(gated.reshape(tokens, N_TP, group_width), (1, 0, 2))
    weight_groups = out_weight.reshape(N_TP, group_width, width)

    def add_group(total, group_items):
        term = jnp.dot(group_items[0], group_items[1], preferred_element_type=jnp.float32).astype(jnp.bfloat16)
        term = lax.optimization_barrier(term)
        return (total + term.astype(jnp.float32), None)
    summed, unused = lax.scan(add_group, jnp.zeros((tokens, width), jnp.float32), (gated_groups, weight_groups))
    stream = (residual.astype(jnp.float32) + summed).astype(jnp.bfloat16)
    stream_f = stream.astype(jnp.float32)
    row_scale = lax.rsqrt(lax.optimization_barrier(jnp.mean(stream_f * stream_f, axis=-1, keepdims=True)) + eps_norm)
    normed_rows = (stream_f * row_scale * norm_gain).astype(jnp.bfloat16)
    block = tokens // N_SP
    group_ids = route_ids.reshape(N_SP, block * TOP)
    one_hot = (group_ids[:, :, None] == jnp.arange(EXPERTS, dtype=jnp.int32)[None, None, :]).astype(jnp.int32)
    slot_rank = lax.optimization_barrier(jnp.sum((jnp.cumsum(one_hot, axis=1) - 1) * one_hot, axis=2))
    group_index = jnp.arange(N_SP, dtype=jnp.int32)[:, None]
    slot_index = (group_ids * (N_SP * CAP) + group_index * CAP + slot_rank).reshape(-1).astype(jnp.int32)
    owner_rows = (jnp.arange(tokens * TOP, dtype=jnp.int32) // TOP).astype(jnp.int32)
    slot_rows = jnp.full((EXPERTS * N_SP * CAP,), tokens, jnp.int32).at[slot_index].set(owner_rows)
    padded_rows = jnp.concatenate([normed_rows, jnp.zeros((1, width), jnp.bfloat16)], axis=0)

    def expert(expert_items):
        rows_index, gate_weight, up_weight, down_weight = expert_items
        rows = padded_rows[rows_index]
        gate_sum = jnp.minimum(jnp.dot(rows, gate_weight, preferred_element_type=jnp.float32), limit_value)
        up_sum = jnp.clip(jnp.dot(rows, up_weight, preferred_element_type=jnp.float32), -limit_value, limit_value)
        active = (gate_sum * jax.nn.sigmoid(alpha_value * gate_sum) * (up_sum + 1.0)).astype(jnp.bfloat16)
        return jnp.dot(active, down_weight, preferred_element_type=jnp.float32).astype(jnp.bfloat16)
    produced = lax.map(expert, (slot_rows.reshape(EXPERTS, N_SP * CAP), w_gate, w_up, w_down))
    picked = produced.reshape(EXPERTS * N_SP * CAP, width)[slot_index].astype(jnp.float32).reshape(tokens, TOP, width)
    moe_out = lax.optimization_barrier(jnp.sum(picked * route_weights[:, :, None], axis=1))
    return (stream_f + moe_out).astype(jnp.bfloat16)
```

```python
import jax
import jax.numpy as jnp
from jax import lax
from jax.experimental import pallas as pl
from jax.experimental.pallas import tpu as pltpu
from jax.sharding import Mesh
from jax.sharding import PartitionSpec as P

F32 = jnp.float32
BF16 = jnp.bfloat16
HI = lax.Precision.HIGHEST
EPS = 1e-06
CAP = 36
PAIR = 2 * CAP
Z = 16
R = 192
W = 128
D = 2048
SLOTS = 1152
SIDE = 4
TP = SIDE * SIDE
HID = 256
SP = ("z", "c")
PLANE = ("y", "x")
CYX = ("c", "y", "x")


def place(c, y, x):
    return (c * SIDE + y) * SIDE + x


FOUR = range(SIDE)
FIRST = [[place(0, y, x) for x in FOUR] for y in FOUR] + [
    [place(1, y, x) for y in FOUR] for x in FOUR
]
SECOND = [[place(0, y, x) for y in FOUR] for x in FOUR] + [
    [place(1, y, x) for x in FOUR] for y in FOUR
]


def exchange(pieces, groups):
    return lax.all_to_all(pieces, CYX, 0, 0, axis_index_groups=groups, tiled=True)


def spread(x, groups):
    return exchange(jnp.broadcast_to(x, (SIDE, *x.shape)), groups)


def dot(a, b, dims, precision=None):
    return lax.dot_general(a, b, (dims, ((), ())), precision=precision, preferred_element_type=F32)


def iota2(shape, dim):
    return lax.broadcasted_iota(jnp.int32, shape, dim)


def head_body(q_ref, v_ref, ff_ref, fb_ref, jr_ref, jc_ref, gap_ref, local_ref, qs_ref, sum_ref):
    q = q_ref[...].astype(F32)
    q = q * jax.nn.sigmoid(q)
    v = v_ref[...].astype(F32)
    row = iota2((R, R), 0)
    col = iota2((R, R), 1)
    jr = jr_ref[...]
    jc = jc_ref[...]
    total = None
    for d, f_ref in enumerate((ff_ref, fb_ref)):
        seen = (col <= row) if d == 0 else (col >= row)
        seen_t = (row <= col) if d == 0 else (row >= col)
        key = gap_ref[d : d + 1, :] * jax.nn.sigmoid(-f_ref[...].astype(F32))
        sums = dot(seen.astype(F32), jnp.log1p(-key), ((1,), (0,)), HI)
        jump_c = jnp.sum(jnp.where(seen, jr, 0.0), axis=1, keepdims=True)
        jump_r = jnp.sum(jnp.where(seen_t, jc, 0.0), axis=0, keepdims=True)
        mid = sums[R // 2 : R // 2 + 1, :]
        scores = dot(q * jnp.exp(sums - mid), key * jnp.exp(mid - sums), ((1,), (1,)), HI)
        fade = jnp.exp(jnp.where(seen, jump_c - jump_r, -1e30))
        part = dot(scores * fade, v, ((1,), (0,)), HI)
        total = part if total is None else total + part
        last = R - 1 if d == 0 else 0
        end = sums[last : last + 1, :]
        end_jump = jump_c[last : last + 1, :]
        key_end = key * jnp.exp((end - sums) + (end_jump - jump_c))
        sum_ref[d, 0:W, :] = dot(v, key_end, ((0,), (0,)), HI)
        sum_ref[d, W : W + 8, :] = jnp.broadcast_to(jnp.exp(end + end_jump), (8, W))
        qs_ref[d] = q * jnp.exp(sums + jump_c)
    local_ref[...] = total


def pack_body(at_ref, sum_ref, out_ref):
    z = at_ref[0]
    c = at_ref[1]
    start = pl.multiple_of(c * (W // 2), W // 2)

    def message(d):
        near, far = (1, 0) if d == 0 else (0, 1)
        near_decay = sum_ref[near, d, W : W + 1, :]
        decay = sum_ref[far, d, W : W + 1, :] * near_decay
        state = (
            sum_ref[far, d, pl.ds(start, W // 2), :] * near_decay
            + sum_ref[near, d, pl.ds(start, W // 2), :]
        )
        high = decay.astype(BF16).astype(F32)
        low = decay - high
        line = iota2((8, W), 0)
        tail = jnp.where(line == 0, high, jnp.where(line == 1, low, 0.0))
        return jnp.concatenate([state, tail], axis=0).astype(BF16)

    fwd = message(0)
    bwd = message(1)
    for k in range(Z):
        later = jnp.full((W // 2 + 8, W), k, jnp.int32) > z
        out_ref[k] = jnp.where(later, fwd.astype(F32), bwd.astype(F32)).astype(BF16)


def carry_body(at_ref, got_ref, out_ref):
    z = at_ref[0]

    def step(k, carry):
        got = got_ref[k].astype(F32)
        return carry * (got[W // 2 : W // 2 + 1] + got[W // 2 + 1 : W // 2 + 2]) + got[: W // 2]

    zero = jnp.zeros((W // 2, W), F32)
    out_ref[0] = lax.fori_loop(0, z, step, zero)
    out_ref[1] = lax.fori_loop(0, Z - 1 - z, lambda k, s: step(Z - 1 - k, s), zero)


def mix_body(at_ref, local_ref, qs_ref, sum_ref, carry_ref, gate_ref, gain_ref, w_ref, out_ref):
    c = at_ref[1]
    o = local_ref[...]
    for d in range(2):
        carry = jnp.concatenate([carry_ref[0, d], carry_ref[1, d]], axis=0)
        through = carry * sum_ref[d, d, W : W + 1, :] + sum_ref[d, d, 0:W, :]
        passed = jnp.full((W, W), c, jnp.int32) != d
        o = o + dot(qs_ref[d], jnp.where(passed, through, carry), ((1,), (1,)), HI)
    mean_square = jnp.mean(o * o, axis=1, keepdims=True)
    gate = gate_ref[...].astype(F32)
    gated = o * lax.rsqrt(mean_square + EPS) * gain_ref[...] * (gate * jax.nn.sigmoid(gate))
    terms = dot(gated.astype(BF16), w_ref[...], ((1,), (0,))).astype(BF16)
    for k in range(TP):
        out_ref[k] = terms[:, k * W : (k + 1) * W]


def slots_of(ids):
    expert = iota2((32, R), 0)
    named = ids[0:1] == expert
    for j in range(1, 4):
        named = named | (ids[j : j + 1] == expert)
    before = (iota2((R, R), 0) < iota2((R, R), 1)).astype(BF16)
    rank = dot(named.astype(BF16), before, ((1,), (0,)))
    return jnp.where(named, rank, -1000.0)


def send_body(at_ref, got_ref, res_ref, ids_ref, stream_ref, out_ref):
    total = got_ref[0].astype(F32)
    for k in range(1, TP):
        total = total + got_ref[k].astype(F32)
    stream = (res_ref[...].astype(F32) + total).astype(BF16)
    stream_ref[...] = stream
    slots = slots_of(ids_ref[...])
    line = iota2((PAIR, R), 0).astype(F32)
    for z in range(Z):
        hit = (line == slots[2 * z : 2 * z + 1]) | (line == slots[2 * z + 1 : 2 * z + 2] + CAP)
        out_ref[z] = dot(hit.astype(BF16), stream, ((1,), (0,))).astype(BF16)


def up_body(perm_ref, x_ref, gain_ref, wg_ref, wu_ref, out_ref, rows_ref):
    squares = None
    for j in range(TP):
        x = x_ref[perm_ref[j]].astype(F32)
        part = x * x
        squares = part if squares is None else squares + part
    scale = lax.rsqrt(jnp.sum(squares, axis=1, keepdims=True) / D + EPS)
    for j in range(TP):
        x = x_ref[perm_ref[j]].astype(F32)
        cols = pl.ds(j * W, W)
        rows_ref[:, cols] = (x * scale * gain_ref[:, cols]).astype(BF16)
    rows = rows_ref[...]
    c = jnp.minimum(dot(rows, wg_ref[...], ((1,), (0,))), 7.0)
    u = jnp.clip(dot(rows, wu_ref[...], ((1,), (0,))), -7.0, 7.0)
    active = (c * jax.nn.sigmoid(1.702 * c) * (u + 1.0)).astype(BF16)
    for k in range(SIDE):
        out_ref[k] = active


def down_body(act_ref, w_ref, out_ref, whole_ref):
    @pl.when(pl.program_id(0) == 0)
    def _():
        for k in range(SIDE):
            whole_ref[:, k * W : (k + 1) * W] = w_ref[k]

    active = jnp.concatenate([act_ref[k] for k in range(SIDE)], axis=1)
    made = dot(active, whole_ref[...], ((1,), (0,))).astype(BF16)
    for k in range(SIDE):
        out_ref[k] = made[:, k * W : (k + 1) * W]


def return_body(got_ref, stream_ref, ids_ref, weights_ref, out_ref):
    ids = ids_ref[...]
    weights = weights_ref[...]
    slots = slots_of(ids)
    expert = iota2((32, R), 0)
    share = jnp.where(ids[0:1] == expert, weights[0:1], 0.0)
    for j in range(1, 4):
        share = share + jnp.where(ids[j : j + 1] == expert, weights[j : j + 1], 0.0)
    line = iota2((PAIR, R), 0).astype(F32)
    total = jnp.zeros((R, W), F32)
    for z in range(Z):
        a = slice(2 * z, 2 * z + 1)
        b = slice(2 * z + 1, 2 * z + 2)
        share_at = jnp.where(line == slots[a], share[a], 0.0)
        share_at = share_at + jnp.where(line == slots[b] + CAP, share[b], 0.0)
        high = share_at.astype(BF16)
        low = (share_at - high.astype(F32)).astype(BF16)
        got = got_ref[z]
        total = total + (dot(high, got, ((0,), (0,))) + dot(low, got, ((0,), (0,))))
    out_ref[...] = (stream_ref[...].astype(F32) + total).astype(BF16)


VMEM = pl.BlockSpec(memory_space=pltpu.VMEM)
SMEM = pl.BlockSpec(memory_space=pltpu.SMEM)


def whole(body, outs, specs, name):
    return pl.pallas_call(
        body,
        out_shape=[jax.ShapeDtypeStruct(s, t) for s, t in outs],
        in_specs=specs,
        out_specs=[VMEM] * len(outs),
        name=name,
    )


def shards(
    residual,
    query_in,
    value_in,
    forget_fwd,
    forget_bwd,
    jumps,
    gate_gap,
    out_gate,
    head_gain,
    out_weight,
    norm_gain,
    route_ids,
    route_weights,
    w_gate,
    w_up,
    w_down,
):
    z = lax.axis_index("z")
    c = lax.axis_index("c")
    tp = lax.axis_index(PLANE)
    at = jnp.stack([z, c]).astype(jnp.int32)
    ids = route_ids.T
    weights = route_weights.T

    down = w_down.reshape(SIDE, SIDE, HID, W)
    down = jnp.where(c == 0, down, down.transpose(1, 0, 2, 3)).reshape(SIDE, SIDE * HID, W)
    down = exchange(down, SECOND)

    local, qs, summary = whole(
        head_body,
        (((R, W), F32), ((2, R, W), F32), ((2, W + 8, W), F32)),
        [VMEM] * 7,
        "head",
    )(query_in, value_in, forget_fwd, forget_bwd, jumps, jumps.reshape(R, 1), gate_gap)
    both = lax.all_gather(summary, "c")
    (packed,) = whole(pack_body, (((Z, W // 2 + 8, W), BF16),), [SMEM, VMEM], "pack")(at, both)
    packed = lax.all_to_all(packed, "z", 0, 0, tiled=True)
    (half,) = whole(carry_body, (((2, W // 2, W), F32),), [SMEM, VMEM], "carry")(at, packed)
    carry = lax.all_gather(half, "c")
    (terms,) = whole(mix_body, (((TP, R, W), BF16),), [SMEM] + [VMEM] * 7, "mix")(
        at, local, qs, both, carry, out_gate, head_gain.reshape(1, W), out_weight
    )
    terms = lax.all_to_all(terms, PLANE, 0, 0, tiled=True)

    own_residual = lax.dynamic_slice_in_dim(residual, tp * W, W, 1)
    stream, buffer = whole(
        send_body,
        (((R, W), BF16), ((Z, PAIR, W), BF16)),
        [SMEM] + [VMEM] * 3,
        "send",
    )(at, terms, own_residual, ids)

    arrived = lax.all_to_all(buffer, "z", 0, 0, tiled=True)
    arrived = arrived.reshape(Z, 2, CAP, W).transpose(1, 0, 2, 3).reshape(2, Z * CAP, W)
    rows = lax.all_to_all(arrived, "c", 0, 0, tiled=True).reshape(SLOTS, W)
    rows = spread(spread(rows, FIRST), SECOND).reshape(TP, SLOTS, W)

    j = jnp.arange(TP, dtype=jnp.int32)
    perm = jnp.where(c == 0, j, (j % SIDE) * SIDE + j // SIDE)
    step = 192
    active = pl.pallas_call(
        up_body,
        grid_spec=pltpu.PrefetchScalarGridSpec(
            num_scalar_prefetch=1,
            grid=(SLOTS // step,),
            in_specs=[
                pl.BlockSpec((TP, step, W), lambda i, p: (0, i, 0)),
                pl.BlockSpec((1, D), lambda i, p: (0, 0)),
                pl.BlockSpec((D, HID), lambda i, p: (0, 0)),
                pl.BlockSpec((D, HID), lambda i, p: (0, 0)),
            ],
            out_specs=pl.BlockSpec((SIDE, step, HID), lambda i, p: (0, i, 0)),
            scratch_shapes=[pltpu.VMEM((step, D), BF16)],
        ),
        out_shape=jax.ShapeDtypeStruct((SIDE, SLOTS, HID), BF16),
        name="up",
    )(perm, rows, norm_gain.reshape(1, D), w_gate[0], w_up[0])

    active = exchange(active, FIRST)
    made = pl.pallas_call(
        down_body,
        grid=(SLOTS // step,),
        in_specs=[
            pl.BlockSpec((SIDE, step, HID), lambda i: (0, i, 0)),
            pl.BlockSpec((SIDE, SIDE * HID, W), lambda i: (0, 0, 0)),
        ],
        out_specs=pl.BlockSpec((SIDE, step, W), lambda i: (0, i, 0)),
        out_shape=jax.ShapeDtypeStruct((SIDE, SLOTS, W), BF16),
        scratch_shapes=[pltpu.VMEM((SIDE * HID, SIDE * W), BF16)],
        name="down",
    )(active, down)
    made = exchange(made, SECOND)
    produced = jnp.sum(made.astype(F32), axis=0).astype(BF16)

    back = lax.all_to_all(produced.reshape(2, Z * CAP, W), "c", 0, 0, tiled=True)
    back = back.reshape(2, Z, CAP, W).transpose(1, 0, 2, 3).reshape(Z, PAIR, W)
    back = lax.all_to_all(back, "z", 0, 0, tiled=True)
    (mixed,) = whole(return_body, (((R, W), BF16),), [VMEM] * 4, "back")(
        back, stream, ids, weights
    )
    return mixed


def solution(mesh):
    finer = Mesh(mesh.devices.reshape(Z, 2, SIDE, SIDE), ("z", "c", "y", "x"))
    return jax.shard_map(
        shards,
        mesh=finer,
        in_specs=(
            P(SP, None),
            P(SP, PLANE),
            P(SP, PLANE),
            P(SP, PLANE),
            P(SP, PLANE),
            P(PLANE, SP),
            P(None, PLANE),
            P(SP, PLANE),
            P(PLANE),
            P(PLANE, None),
            P(),
            P(SP, None),
            P(SP, None),
            P(SP, None, PLANE),
            P(SP, None, PLANE),
            P(SP, None, PLANE),
        ),
        out_specs=P(SP, PLANE),
        check_vma=False,
    )
```

```python
import jax
import jax.numpy as jnp
from jax import lax
from jax.experimental import pallas as pl
from jax.experimental.pallas import tpu as pltpu
from jax.sharding import Mesh
from jax.sharding import PartitionSpec as P

F32 = jnp.float32
BF16 = jnp.bfloat16
EPS = 1e-06
CAP = 36
PAIR = 2 * CAP
Z = 16
R = 192
W = 128
D = 2048
SLOTS = 1152
SIDE = 4
TP = SIDE * SIDE
HID = 256
SP = ("z", "c")
PLANE = ("y", "x")
CYX = ("c", "y", "x")


def place(c, y, x):
    return (c * SIDE + y) * SIDE + x


FOUR = range(SIDE)
FIRST = [[place(0, y, x) for x in FOUR] for y in FOUR] + [
    [place(1, y, x) for y in FOUR] for x in FOUR
]
SECOND = [[place(0, y, x) for y in FOUR] for x in FOUR] + [
    [place(1, y, x) for x in FOUR] for y in FOUR
]


def exchange(pieces, groups):
    return lax.all_to_all(pieces, CYX, 0, 0, axis_index_groups=groups, tiled=True)


def dot(a, b, dims):
    return lax.dot_general(a, b, (dims, ((), ())), preferred_element_type=F32)


def split(a):
    high = a.astype(BF16)
    return high, (a - high.astype(F32)).astype(BF16)


def dot2(a, b, dims):
    high, low = split(a)
    return dot(high, b, dims) + dot(low, b, dims)


def dot3(a, b, dims):
    ah, al = split(a)
    bh, bl = split(b)
    return dot(ah, bh, dims) + (dot(ah, bl, dims) + dot(al, bh, dims))


def iota2(shape, dim):
    return lax.broadcasted_iota(jnp.int32, shape, dim)


def head_body(
    at_ref,
    q_hbm,
    v_hbm,
    ff_hbm,
    fb_hbm,
    jr_hbm,
    gap_hbm,
    res_hbm,
    local_ref,
    qs_ref,
    sum_ref,
    res_ref,
    q_ref,
    v_ref,
    ff_ref,
    fb_ref,
    jr_ref,
    gap_ref,
    sems,
):
    own = pl.ds(pl.multiple_of(at_ref[2] * W, W), W)
    moves = (
        (q_hbm, q_ref),
        (ff_hbm, ff_ref),
        (jr_hbm, jr_ref),
        (gap_hbm, gap_ref),
        (v_hbm, v_ref),
        (fb_hbm, fb_ref),
        (res_hbm.at[:, own], res_ref),
    )
    copies = [pltpu.make_async_copy(a, b, sems.at[k]) for k, (a, b) in enumerate(moves)]
    for copy in copies:
        copy.start()
    for copy in copies:
        copy.wait()
    q = q_ref[...].astype(F32)
    q = q * jax.nn.sigmoid(q)
    v = v_ref[...]
    row = iota2((R, R), 0)
    col = iota2((R, R), 1)
    jr = jr_ref[...]
    jc = jnp.sum(jnp.where(row == col, jr, 0.0), axis=1, keepdims=True)
    total = None
    for d, f_ref in enumerate((ff_ref, fb_ref)):
        seen = (col <= row) if d == 0 else (col >= row)
        seen_t = (row <= col) if d == 0 else (row >= col)
        key = gap_ref[d : d + 1, :] * jax.nn.sigmoid(-f_ref[...].astype(F32))
        high, low = split(jnp.log1p(-key))
        ones = seen.astype(BF16)
        sums = dot(ones, high, ((1,), (0,))) + dot(ones, low, ((1,), (0,)))
        jump_c = jnp.sum(jnp.where(seen, jr, 0.0), axis=1, keepdims=True)
        jump_r = jnp.sum(jnp.where(seen_t, jc, 0.0), axis=0, keepdims=True)
        mid = sums[R // 2 : R // 2 + 1, :]
        scores = dot3(q * jnp.exp(sums - mid), key * jnp.exp(mid - sums), ((1,), (1,)))
        fade = jnp.exp(jnp.where(seen, jump_c - jump_r, -1e30))
        part = dot2(scores * fade, v, ((1,), (0,)))
        total = part if total is None else total + part
        last = R - 1 if d == 0 else 0
        end = sums[last : last + 1, :]
        end_jump = jump_c[last : last + 1, :]
        key_end = key * jnp.exp((end - sums) + (end_jump - jump_c))
        high, low = split(key_end)
        sum_ref[d, 0:W, :] = dot(v, high, ((0,), (0,))) + dot(v, low, ((0,), (0,)))
        sum_ref[d, W : W + 8, :] = jnp.broadcast_to(jnp.exp(end + end_jump), (8, W))
        qs_ref[d] = q * jnp.exp(sums + jump_c)
    local_ref[...] = total


def pack_body(at_ref, sum_ref, out_ref):
    z = at_ref[0]
    c = at_ref[1]
    start = pl.multiple_of(c * (W // 2), W // 2)

    def message(d):
        near, far = (1, 0) if d == 0 else (0, 1)
        near_decay = sum_ref[near, d, W : W + 1, :]
        decay = sum_ref[far, d, W : W + 1, :] * near_decay
        state = (
            sum_ref[far, d, pl.ds(start, W // 2), :] * near_decay
            + sum_ref[near, d, pl.ds(start, W // 2), :]
        )
        high = decay.astype(BF16).astype(F32)
        low = decay - high
        line = iota2((8, W), 0)
        tail = jnp.where(line == 0, high, jnp.where(line == 1, low, 0.0))
        return jnp.concatenate([state, tail], axis=0).astype(BF16)

    fwd = message(0)
    bwd = message(1)
    for k in range(Z):
        later = jnp.full((W // 2 + 8, W), k, jnp.int32) > z
        out_ref[k] = jnp.where(later, fwd.astype(F32), bwd.astype(F32)).astype(BF16)


def carry_body(at_ref, got_ref, out_ref):
    z = at_ref[0]

    def step(k, carry):
        got = got_ref[k].astype(F32)
        return carry * (got[W // 2 : W // 2 + 1] + got[W // 2 + 1 : W // 2 + 2]) + got[: W // 2]

    zero = jnp.zeros((W // 2, W), F32)
    out_ref[0] = lax.fori_loop(0, z, step, zero)
    out_ref[1] = lax.fori_loop(0, Z - 1 - z, lambda k, s: step(Z - 1 - k, s), zero)


def mix_body(at_ref, local_ref, qs_ref, sum_ref, carry_ref, gate_ref, gain_ref, w_ref, out_ref):
    c = at_ref[1]
    o = local_ref[...]
    for d in range(2):
        carry = jnp.concatenate([carry_ref[0, d], carry_ref[1, d]], axis=0)
        through = carry * sum_ref[d, d, W : W + 1, :] + sum_ref[d, d, 0:W, :]
        passed = jnp.full((W, W), c, jnp.int32) != d
        o = o + dot3(qs_ref[d], jnp.where(passed, through, carry), ((1,), (1,)))
    mean_square = jnp.mean(o * o, axis=1, keepdims=True)
    gate = gate_ref[...].astype(F32)
    gated = o * lax.rsqrt(mean_square + EPS) * gain_ref[...] * (gate * jax.nn.sigmoid(gate))
    terms = dot(gated.astype(BF16), w_ref[...], ((1,), (0,))).astype(BF16)
    for k in range(TP):
        out_ref[k] = terms[:, k * W : (k + 1) * W]


def slots_of(ids, expert):
    named = ids[0:1] == expert
    for j in range(1, 4):
        named = named | (ids[j : j + 1] == expert)
    before = (iota2((R, R), 0) < iota2((R, R), 1)).astype(BF16)
    rank = dot(named.astype(BF16), before, ((1,), (0,)))
    return jnp.where(named, rank, -1000.0)


def send_body(at_ref, got_ref, res_ref, ids_ref, stream_ref, out_ref):
    total = got_ref[0].astype(F32)
    for k in range(1, TP):
        total = total + got_ref[k].astype(F32)
    stream = (res_ref[...].astype(F32) + total).astype(BF16)
    stream_ref[...] = stream
    slots = slots_of(ids_ref[...], iota2((32, R), 0))
    line = iota2((PAIR, R), 0).astype(F32)
    for z in range(Z):
        hit = (line == slots[2 * z : 2 * z + 1]) | (line == slots[2 * z + 1 : 2 * z + 2] + CAP)
        out_ref[z] = dot(hit.astype(BF16), stream, ((1,), (0,))).astype(BF16)


def pick_body(at_ref, got_ref, wg_hbm, wu_hbm, out_ref, wg_ref, wu_ref, sems):
    c = at_ref[1]
    copies = [
        pltpu.make_async_copy(wg_hbm, wg_ref, sems.at[0]),
        pltpu.make_async_copy(wu_hbm, wu_ref, sems.at[1]),
    ]
    for copy in copies:
        copy.start()
    line = iota2((PAIR, 2 * PAIR), 0)
    source = iota2((PAIR, 2 * PAIR), 1)
    wanted = line + c * CAP + jnp.where(line < CAP, 0, PAIR - CAP)
    choose = (source == wanted).astype(BF16)
    for z in range(Z):
        both = jnp.concatenate([got_ref[0, z], got_ref[1, z]], axis=0)
        rows = dot(choose, both, ((1,), (0,))).astype(BF16)
        for k in range(SIDE):
            out_ref[k, z * PAIR : (z + 1) * PAIR, :] = rows
    for copy in copies:
        copy.wait()


def fan_body(at_ref, got_ref, wd_hbm, out_ref, sems):
    turned = at_ref[1] == 1
    copies = []
    for k in range(TP):
        a, b = divmod(k, SIDE)
        source = jnp.where(turned, b * SIDE + a, k)
        rows = pl.ds(pl.multiple_of(source * HID, HID), HID)
        target = out_ref.at[a, pl.ds(SIDE * SLOTS + b * HID, HID)]
        copies.append(pltpu.make_async_copy(wd_hbm.at[rows], target, sems.at[k]))
    for copy in copies:
        copy.start()
    for k in range(SIDE):
        rows = got_ref[k]
        for other in range(SIDE):
            out_ref[other, k * SLOTS : (k + 1) * SLOTS] = rows
    for copy in copies:
        copy.wait()


def up_body(at_ref, x0_ref, x1_ref, x2_ref, x3_ref, gain_ref, wg_ref, wu_ref, out_ref, rows_ref):
    turned = at_ref[1] == 1
    parts = (x0_ref, x1_ref, x2_ref, x3_ref)
    squares = None
    for x_ref in parts:
        for a in range(SIDE):
            x = x_ref[a].astype(F32)
            squares = x * x if squares is None else squares + x * x
    scale = lax.rsqrt(jnp.sum(squares, axis=1, keepdims=True) / D + EPS)
    for b, x_ref in enumerate(parts):
        for a in range(SIDE):
            share = jnp.where(turned, b * SIDE + a, a * SIDE + b)
            cols = pl.ds(pl.multiple_of(share * W, W), W)
            x = x_ref[a].astype(F32)
            rows_ref[:, cols] = (x * scale * gain_ref[:, cols]).astype(BF16)
    rows = rows_ref[...]
    c = jnp.minimum(dot(rows, wg_ref[...], ((1,), (0,))), 7.0)
    u = jnp.clip(dot(rows, wu_ref[...], ((1,), (0,))), -7.0, 7.0)
    active = (c * jax.nn.sigmoid(1.702 * c) * (u + 1.0)).astype(BF16)
    for k in range(SIDE):
        out_ref[k] = active


def down_body(act_ref, w0_ref, w1_ref, out_ref, whole_ref):
    @pl.when(pl.program_id(0) == 0)
    def _():
        half = SIDE * HID // 2
        for k in range(SIDE):
            whole_ref[:half, k * W : (k + 1) * W] = w0_ref[k]
            whole_ref[half:, k * W : (k + 1) * W] = w1_ref[k]

    active = jnp.concatenate([act_ref[k] for k in range(SIDE)], axis=1)
    made = dot(active, whole_ref[...], ((1,), (0,))).astype(BF16)
    for k in range(SIDE):
        out_ref[k] = made[:, k * W : (k + 1) * W]


def return_body(at_ref, got_ref, stream_ref, ids_ref, weights_ref, out_ref):
    ids = ids_ref[...]
    weights = weights_ref[...]
    group = iota2((32, R), 0)
    expert = jnp.where(group < Z, 2 * group, 2 * group - 31)
    slots = slots_of(ids, expert)
    share = jnp.where(ids[0:1] == expert, weights[0:1], 0.0)
    for j in range(1, 4):
        share = share + jnp.where(ids[j : j + 1] == expert, weights[j : j + 1], 0.0)
    line = iota2((32, 32 * PAIR), 1)
    first = iota2((32, 32 * PAIR), 0) * PAIR
    inside = (line >= first) & (line < first + PAIR)
    spread = inside.astype(BF16)
    place_in = jnp.sum(jnp.where(inside, line - first, 0), axis=0, keepdims=True)
    rank = (place_in - at_ref[1] * CAP).astype(F32)
    high, low = split(share)
    slot_at = dot(slots.astype(BF16), spread, ((0,), (0,)))
    share_at = dot(high, spread, ((0,), (0,))) + dot(low, spread, ((0,), (0,)))
    mixing = jnp.where(slot_at == rank, share_at, 0.0)
    got = jnp.concatenate([got_ref[k, z] for k in range(2) for z in range(Z)], axis=0)
    total = dot2(mixing, got, ((1,), (0,)))
    out_ref[...] = (stream_ref[...].astype(F32) + total).astype(BF16)


def limit(mib):
    return pltpu.CompilerParams(vmem_limit_bytes=mib << 20)


VMEM = pl.BlockSpec()
SMEM = pl.BlockSpec(memory_space=pltpu.SMEM)
HBM = pl.BlockSpec(memory_space=pltpu.HBM)
IN_VMEM = pl.BlockSpec(memory_space=pltpu.VMEM)


def in_hbm(x):
    return pltpu.with_memory_space_constraint(x, pltpu.HBM)


def whole(body, outs, specs, name):
    return pl.pallas_call(
        body,
        out_shape=[jax.ShapeDtypeStruct(s, t) for s, t in outs],
        in_specs=specs,
        out_specs=[VMEM] * len(outs),
        compiler_params=limit(12),
        name=name,
    )


def share_of_rows(b, step):
    return pl.BlockSpec((SIDE, step, W), lambda i, p: (0, b * (SLOTS // step) + i, 0))


def shards(
    residual,
    query_in,
    value_in,
    forget_fwd,
    forget_bwd,
    jumps,
    gate_gap,
    out_gate,
    head_gain,
    out_weight,
    norm_gain,
    route_ids,
    route_weights,
    w_gate,
    w_up,
    w_down,
):
    z = lax.axis_index("z")
    c = lax.axis_index("c")
    tp = lax.axis_index(PLANE)
    at = jnp.stack([z, c, tp]).astype(jnp.int32)
    ids = route_ids.T
    weights = route_weights.T

    local, qs, summary, own_residual = pl.pallas_call(
        head_body,
        out_shape=[
            jax.ShapeDtypeStruct((R, W), F32),
            jax.ShapeDtypeStruct((2, R, W), F32),
            jax.ShapeDtypeStruct((2, W + 8, W), F32),
            jax.ShapeDtypeStruct((R, W), BF16),
        ],
        in_specs=[SMEM] + [HBM] * 7,
        out_specs=[VMEM] * 4,
        scratch_shapes=[pltpu.VMEM((R, W), BF16)] * 4
        + [pltpu.VMEM((1, R), F32), pltpu.VMEM((2, W), F32), pltpu.SemaphoreType.DMA((7,))],
        compiler_params=limit(8),
        name="head",
    )(
        at,
        *(
            in_hbm(x)
            for x in (query_in, value_in, forget_fwd, forget_bwd, jumps, gate_gap, residual)
        ),
    )
    both = lax.all_gather(summary, "c")
    (packed,) = whole(pack_body, (((Z, W // 2 + 8, W), BF16),), [SMEM, VMEM], "pack")(at, both)
    packed = lax.all_to_all(packed, "z", 0, 0, tiled=True)
    (half,) = whole(carry_body, (((2, W // 2, W), F32),), [SMEM, VMEM], "carry")(at, packed)
    carry = lax.all_gather(half, "c")
    (terms,) = whole(mix_body, (((TP, R, W), BF16),), [SMEM] + [VMEM] * 7, "mix")(
        at, local, qs, both, carry, out_gate, head_gain.reshape(1, W), out_weight
    )
    terms = lax.all_to_all(terms, PLANE, 0, 0, tiled=True)

    stream, buffer = whole(
        send_body,
        (((R, W), BF16), ((Z, PAIR, W), BF16)),
        [SMEM] + [VMEM] * 3,
        "send",
    )(at, terms, own_residual, ids)

    arrived = lax.all_to_all(buffer, "z", 0, 0, tiled=True)
    arrived = lax.all_gather(arrived, "c")
    rows, gate_w, up_w = pl.pallas_call(
        pick_body,
        out_shape=[
            jax.ShapeDtypeStruct((SIDE, SLOTS, W), BF16),
            pltpu.VMEM((D, HID), BF16),
            pltpu.VMEM((D, HID), BF16),
        ],
        in_specs=[SMEM, VMEM, HBM, HBM],
        out_specs=[VMEM, IN_VMEM, IN_VMEM],
        scratch_shapes=[pltpu.SemaphoreType.DMA((2,))],
        compiler_params=limit(12),
        name="pick",
    )(at, arrived, in_hbm(w_gate[0]), in_hbm(w_up[0]))
    rows = exchange(rows, FIRST)
    rows = pl.pallas_call(
        fan_body,
        out_shape=jax.ShapeDtypeStruct((SIDE, SIDE * (SLOTS + HID), W), BF16),
        in_specs=[SMEM, VMEM, HBM],
        out_specs=VMEM,
        scratch_shapes=[pltpu.SemaphoreType.DMA((TP,))],
        compiler_params=limit(16),
        name="fan",
    )(at, rows, in_hbm(w_down[0]))
    rows = exchange(rows, SECOND)

    step = 576
    active = pl.pallas_call(
        up_body,
        grid_spec=pltpu.PrefetchScalarGridSpec(
            num_scalar_prefetch=1,
            grid=(SLOTS // step,),
            in_specs=[
                *(share_of_rows(b, step) for b in range(SIDE)),
                pl.BlockSpec((1, D), lambda i, p: (0, 0)),
                pl.BlockSpec((D, HID), lambda i, p: (0, 0)),
                pl.BlockSpec((D, HID), lambda i, p: (0, 0)),
            ],
            out_specs=pl.BlockSpec((SIDE, step, HID), lambda i, p: (0, i, 0)),
            scratch_shapes=[pltpu.VMEM((step, D), BF16)],
        ),
        out_shape=jax.ShapeDtypeStruct((SIDE, SLOTS, HID), BF16),
        compiler_params=limit(24),
        name="up",
    )(at, rows, rows, rows, rows, norm_gain.reshape(1, D), gate_w, up_w)

    active = exchange(active, FIRST)
    made = pl.pallas_call(
        down_body,
        grid=(SLOTS // step,),
        in_specs=[
            pl.BlockSpec((SIDE, step, HID), lambda i: (0, i, 0)),
            pl.BlockSpec((SIDE, 2 * HID, W), lambda i: (0, 9, 0)),
            pl.BlockSpec((SIDE, 2 * HID, W), lambda i: (0, 10, 0)),
        ],
        out_specs=pl.BlockSpec((SIDE, step, W), lambda i: (0, i, 0)),
        out_shape=jax.ShapeDtypeStruct((SIDE, SLOTS, W), BF16),
        scratch_shapes=[pltpu.VMEM((SIDE * HID, SIDE * W), BF16)],
        compiler_params=limit(16),
        name="down",
    )(active, rows, rows)
    made = exchange(made, SECOND)
    produced = jnp.sum(made.astype(F32), axis=0).astype(BF16)

    back = lax.all_to_all(produced.reshape(Z, PAIR, W), "z", 0, 0, tiled=True)
    back = lax.all_gather(back, "c")
    (mixed,) = whole(return_body, (((R, W), BF16),), [SMEM] + [VMEM] * 4, "back")(
        at, back, stream, ids, weights
    )
    return mixed


def solution(mesh):
    finer = Mesh(mesh.devices.reshape(Z, 2, SIDE, SIDE), ("z", "c", "y", "x"))
    return jax.shard_map(
        shards,
        mesh=finer,
        in_specs=(
            P(SP, None),
            P(SP, PLANE),
            P(SP, PLANE),
            P(SP, PLANE),
            P(SP, PLANE),
            P(PLANE, SP),
            P(None, PLANE),
            P(SP, PLANE),
            P(PLANE),
            P(PLANE, None),
            P(),
            P(SP, None),
            P(SP, None),
            P(SP, None, PLANE),
            P(SP, None, PLANE),
            P(SP, None, PLANE),
        ),
        out_specs=P(SP, PLANE),
        check_vma=False,
    )
```

```python
import jax
import jax.numpy as jnp
from jax import lax
from jax.experimental import pallas as pl
from jax.experimental.pallas import tpu as pltpu
from jax.sharding import Mesh
from jax.sharding import PartitionSpec as P

F32 = jnp.float32
BF16 = jnp.bfloat16
EPS = 1e-06
CAP = 36
PAIR = 2 * CAP
Z = 16
R = 192
W = 128
D = 2048
SLOTS = 1152
PART = 288
SIDE = 4
TP = SIDE * SIDE
HID = 256
SP = ("z", "c")
PLANE = ("y", "x")
CYX = ("c", "y", "x")


def place(c, y, x):
    return (c * SIDE + y) * SIDE + x


FOUR = range(SIDE)
FIRST = [[place(0, y, x) for x in FOUR] for y in FOUR] + [
    [place(1, y, x) for y in FOUR] for x in FOUR
]
SECOND = [[place(0, y, x) for y in FOUR] for x in FOUR] + [
    [place(1, y, x) for x in FOUR] for y in FOUR
]


def exchange(pieces, groups):
    return lax.all_to_all(pieces, CYX, 0, 0, axis_index_groups=groups, tiled=True)


def ring(step):
    return [
        (place(c, y, x), place(c, (y + step * c) % SIDE, (x + step * (1 - c)) % SIDE))
        for c in range(2)
        for y in FOUR
        for x in FOUR
    ]


def passed_on(x, step):
    return lax.ppermute(x, CYX, ring(step))


def dot(a, b, dims):
    return lax.dot_general(a, b, (dims, ((), ())), preferred_element_type=F32)


def split(a):
    high = a.astype(BF16)
    return high, (a - high.astype(F32)).astype(BF16)


def dot2(a, b, dims):
    high, low = split(a)
    return dot(high, b, dims) + dot(low, b, dims)


def dot3(a, b, dims):
    ah, al = split(a)
    bh, bl = split(b)
    return dot(ah, bh, dims) + (dot(ah, bl, dims) + dot(al, bh, dims))


def iota2(shape, dim):
    return lax.broadcasted_iota(jnp.int32, shape, dim)


def head_body(
    at_ref,
    q_hbm,
    v_hbm,
    ff_hbm,
    fb_hbm,
    jr_hbm,
    gap_hbm,
    res_hbm,
    wg_hbm,
    wu_hbm,
    wd_hbm,
    local_ref,
    qs_ref,
    sum_ref,
    res_ref,
    joined_hbm,
    held_ref,
    q_ref,
    v_ref,
    ff_ref,
    fb_ref,
    jr_ref,
    gap_ref,
    sems,
):
    own = pl.ds(pl.multiple_of(at_ref[2] * W, W), W)
    moves = (
        (q_hbm, q_ref),
        (ff_hbm, ff_ref),
        (jr_hbm, jr_ref),
        (gap_hbm, gap_ref),
        (v_hbm, v_ref),
        (fb_hbm, fb_ref),
        (res_hbm.at[:, own], res_ref),
    )
    copies = [pltpu.make_async_copy(a, b, sems.at[k]) for k, (a, b) in enumerate(moves)]
    inward = []
    outward = []
    for k, w_hbm in enumerate((wg_hbm, wg_hbm, wu_hbm, wu_hbm, wd_hbm)):
        source = w_hbm if k == 4 else w_hbm.at[:, pl.ds((k % 2) * W, W)]
        held = held_ref.at[pl.ds(k * D, 2 * D if k == 4 else D)]
        target = joined_hbm.at[pl.ds(k * D, 2 * D if k == 4 else D)]
        inward.append(pltpu.make_async_copy(source, held, sems.at[7 + k]))
        outward.append(pltpu.make_async_copy(held, target, sems.at[12 + k]))
    for copy in copies + inward:
        copy.start()
    for copy in copies:
        copy.wait()
    for first, second in zip(inward, outward):
        first.wait()
        second.start()
    q = q_ref[...].astype(F32)
    q = q * jax.nn.sigmoid(q)
    v = v_ref[...]
    row = iota2((R, R), 0)
    col = iota2((R, R), 1)
    jr = jr_ref[...]
    jc = jnp.sum(jnp.where(row == col, jr, 0.0), axis=1, keepdims=True)
    total = None
    for d, f_ref in enumerate((ff_ref, fb_ref)):
        seen = (col <= row) if d == 0 else (col >= row)
        seen_t = (row <= col) if d == 0 else (row >= col)
        key = gap_ref[d : d + 1, :] * jax.nn.sigmoid(-f_ref[...].astype(F32))
        high, low = split(jnp.log1p(-key))
        ones = seen.astype(BF16)
        sums = dot(ones, high, ((1,), (0,))) + dot(ones, low, ((1,), (0,)))
        jump_c = jnp.sum(jnp.where(seen, jr, 0.0), axis=1, keepdims=True)
        jump_r = jnp.sum(jnp.where(seen_t, jc, 0.0), axis=0, keepdims=True)
        mid = sums[R // 2 : R // 2 + 1, :]
        scores = dot3(q * jnp.exp(sums - mid), key * jnp.exp(mid - sums), ((1,), (1,)))
        fade = jnp.exp(jnp.where(seen, jump_c - jump_r, -1e30))
        part = dot2(scores * fade, v, ((1,), (0,)))
        total = part if total is None else total + part
        last = R - 1 if d == 0 else 0
        end = sums[last : last + 1, :]
        end_jump = jump_c[last : last + 1, :]
        key_end = key * jnp.exp((end - sums) + (end_jump - jump_c))
        high, low = split(key_end)
        sum_ref[d, 0:W, :] = dot(v, high, ((0,), (0,))) + dot(v, low, ((0,), (0,)))
        sum_ref[d, W : W + 8, :] = jnp.broadcast_to(jnp.exp(end + end_jump), (8, W))
        qs_ref[d] = q * jnp.exp(sums + jump_c)
    local_ref[...] = total
    for copy in outward:
        copy.wait()


def pack_body(at_ref, sum_ref, out_ref):
    z = at_ref[0]
    c = at_ref[1]
    start = pl.multiple_of(c * (W // 2), W // 2)

    def message(d):
        near, far = (1, 0) if d == 0 else (0, 1)
        near_decay = sum_ref[near, d, W : W + 1, :]
        decay = sum_ref[far, d, W : W + 1, :] * near_decay
        state = (
            sum_ref[far, d, pl.ds(start, W // 2), :] * near_decay
            + sum_ref[near, d, pl.ds(start, W // 2), :]
        )
        high = decay.astype(BF16).astype(F32)
        low = decay - high
        line = iota2((8, W), 0)
        tail = jnp.where(line == 0, high, jnp.where(line == 1, low, 0.0))
        return jnp.concatenate([state, tail], axis=0).astype(BF16)

    fwd = message(0)
    bwd = message(1)
    for k in range(Z):
        later = jnp.full((W // 2 + 8, W), k, jnp.int32) > z
        out_ref[k] = jnp.where(later, fwd.astype(F32), bwd.astype(F32)).astype(BF16)


def carry_body(at_ref, got_ref, out_ref):
    z = at_ref[0]

    def step(k, carry):
        got = got_ref[k].astype(F32)
        return carry * (got[W // 2 : W // 2 + 1] + got[W // 2 + 1 : W // 2 + 2]) + got[: W // 2]

    zero = jnp.zeros((W // 2, W), F32)
    out_ref[0] = lax.fori_loop(0, z, step, zero)
    out_ref[1] = lax.fori_loop(0, Z - 1 - z, lambda k, s: step(Z - 1 - k, s), zero)


def mix_body(at_ref, local_ref, qs_ref, sum_ref, carry_ref, gate_ref, gain_ref, w_ref, out_ref):
    c = at_ref[1]
    o = local_ref[...]
    for d in range(2):
        carry = jnp.concatenate([carry_ref[0, d], carry_ref[1, d]], axis=0)
        through = carry * sum_ref[d, d, W : W + 1, :] + sum_ref[d, d, 0:W, :]
        passed = jnp.full((W, W), c, jnp.int32) != d
        o = o + dot3(qs_ref[d], jnp.where(passed, through, carry), ((1,), (1,)))
    mean_square = jnp.mean(o * o, axis=1, keepdims=True)
    gate = gate_ref[...].astype(F32)
    gated = o * lax.rsqrt(mean_square + EPS) * gain_ref[...] * (gate * jax.nn.sigmoid(gate))
    terms = dot(gated.astype(BF16), w_ref[...], ((1,), (0,))).astype(BF16)
    for k in range(TP):
        out_ref[k] = terms[:, k * W : (k + 1) * W]


def slots_of(ids, expert):
    named = ids[0:1] == expert
    for j in range(1, 4):
        named = named | (ids[j : j + 1] == expert)
    before = (iota2((R, R), 0) < iota2((R, R), 1)).astype(BF16)
    rank = dot(named.astype(BF16), before, ((1,), (0,)))
    return jnp.where(named, rank, -1000.0)


def send_body(at_ref, got_ref, res_ref, ids_ref, stream_ref, out_ref):
    total = got_ref[0].astype(F32)
    for k in range(1, TP):
        total = total + got_ref[k].astype(F32)
    stream = (res_ref[...].astype(F32) + total).astype(BF16)
    stream_ref[...] = stream
    slots = slots_of(ids_ref[...], iota2((32, R), 0))
    line = iota2((PAIR, R), 0).astype(F32)
    for z in range(Z):
        hit = (line == slots[2 * z : 2 * z + 1]) | (line == slots[2 * z + 1 : 2 * z + 2] + CAP)
        out_ref[z] = dot(hit.astype(BF16), stream, ((1,), (0,))).astype(BF16)


def pick_body(at_ref, got_ref, out_ref):
    c = at_ref[1]
    line = iota2((PAIR, 2 * PAIR), 0)
    source = iota2((PAIR, 2 * PAIR), 1)
    wanted = line + c * CAP + jnp.where(line < CAP, 0, PAIR - CAP)
    choose = (source == wanted).astype(BF16)
    for z in range(Z):
        both = jnp.concatenate([got_ref[0, z], got_ref[1, z]], axis=0)
        out_ref[z * PAIR : (z + 1) * PAIR, :] = dot(choose, both, ((1,), (0,))).astype(BF16)


def up_body(
    at_ref, x_ref, gain_ref, own, plus, minus, far0, far1, out_ref, wd_ref, w_ref, rows_ref, sems
):
    def piece(q, k, rows):
        start = k * D
        if q < 3:
            return (own, plus, minus)[q].at[pl.ds(start, rows)]
        return (far0, far1)[start // (3 * D)].at[pl.ds(start % (3 * D), rows)]

    copies = []
    for q in range(SIDE):
        for k in range(4):
            target = w_ref.at[q, k // 2, :, pl.ds((k % 2) * W, W)]
            copies.append(pltpu.make_async_copy(piece(q, k, D), target, sems.at[5 * q + k]))
    for q in range(SIDE):
        target = wd_ref.at[:, pl.ds(q * W, W)]
        copies.append(pltpu.make_async_copy(piece(q, 4, 2 * D), target, sems.at[5 * q + 4]))
    for copy in copies:
        copy.start()
    turned = at_ref[1] == 1
    squares = None
    for p in range(TP):
        x = x_ref[p].astype(F32)
        squares = x * x if squares is None else squares + x * x
    scale = lax.rsqrt(jnp.sum(squares, axis=1, keepdims=True) / D + EPS)
    for p in range(TP):
        share = jnp.where(turned, (p % SIDE) * SIDE + p // SIDE, p)
        cols = pl.ds(pl.multiple_of(share * W, W), W)
        rows_ref[:, cols] = (x_ref[p].astype(F32) * scale * gain_ref[:, cols]).astype(BF16)
    rows = rows_ref[...]
    for q in range(SIDE):
        for copy in copies[4 * q : 4 * q + 4]:
            copy.wait()
        c = jnp.minimum(dot(rows, w_ref[q, 0], ((1,), (0,))), 7.0)
        u = jnp.clip(dot(rows, w_ref[q, 1], ((1,), (0,))), -7.0, 7.0)
        active = (c * jax.nn.sigmoid(1.702 * c) * (u + 1.0)).astype(BF16)
        for k in range(SIDE):
            out_ref[k, :, q * HID : (q + 1) * HID] = active
    for copy in copies[4 * SIDE :]:
        copy.wait()


def along(at_ref, q):
    a = jnp.where(at_ref[1] == 0, at_ref[2] % SIDE, at_ref[2] // SIDE)
    return (a + (0, SIDE - 1, 1, 2)[q]) % SIDE


def down_body(at_ref, act_ref, w_ref, out_ref):
    made = None
    for q in range(SIDE):
        a = along(at_ref, q)
        for b in range(SIDE):
            share = jnp.where(at_ref[1] == 0, b * SIDE + a, a * SIDE + b)
            w = w_ref[pl.ds(pl.multiple_of(share * HID, HID), HID), :]
            term = dot(act_ref[b, :, q * HID : (q + 1) * HID], w, ((1,), (0,)))
            made = term if made is None else made + term
    made = made.astype(BF16)
    for q in range(SIDE):
        out_ref[along(at_ref, q)] = made[:, q * W : (q + 1) * W]


def return_body(at_ref, got_ref, stream_ref, ids_ref, weights_ref, out_ref):
    ids = ids_ref[...]
    weights = weights_ref[...]
    group = iota2((32, R), 0)
    expert = jnp.where(group < Z, 2 * group, 2 * group - 31)
    slots = slots_of(ids, expert)
    share = jnp.where(ids[0:1] == expert, weights[0:1], 0.0)
    for j in range(1, 4):
        share = share + jnp.where(ids[j : j + 1] == expert, weights[j : j + 1], 0.0)
    line = iota2((32, 32 * PAIR), 1)
    first = iota2((32, 32 * PAIR), 0) * PAIR
    inside = (line >= first) & (line < first + PAIR)
    spread = inside.astype(BF16)
    place_in = jnp.sum(jnp.where(inside, line - first, 0), axis=0, keepdims=True)
    rank = (place_in - at_ref[1] * CAP).astype(F32)
    high, low = split(share)
    slot_at = dot(slots.astype(BF16), spread, ((0,), (0,)))
    share_at = dot(high, spread, ((0,), (0,))) + dot(low, spread, ((0,), (0,)))
    mixing = jnp.where(slot_at == rank, share_at, 0.0)
    got = jnp.concatenate([got_ref[k, z] for k in range(2) for z in range(Z)], axis=0)
    total = dot2(mixing, got, ((1,), (0,)))
    out_ref[...] = (stream_ref[...].astype(F32) + total).astype(BF16)


def limit(mib):
    return pltpu.CompilerParams(vmem_limit_bytes=mib << 20)


VMEM = pl.BlockSpec()
SMEM = pl.BlockSpec(memory_space=pltpu.SMEM)
HBM = pl.BlockSpec(memory_space=pltpu.HBM)
IN_VMEM = pl.BlockSpec(memory_space=pltpu.VMEM)


def in_hbm(x):
    return pltpu.with_memory_space_constraint(x, pltpu.HBM)


def whole(body, outs, specs):
    return pl.pallas_call(
        body,
        out_shape=[jax.ShapeDtypeStruct(s, t) for s, t in outs],
        in_specs=specs,
        out_specs=[VMEM] * len(outs),
        compiler_params=limit(12),
    )


def shards(
    residual,
    query_in,
    value_in,
    forget_fwd,
    forget_bwd,
    jumps,
    gate_gap,
    out_gate,
    head_gain,
    out_weight,
    norm_gain,
    route_ids,
    route_weights,
    w_gate,
    w_up,
    w_down,
):
    z = lax.axis_index("z")
    c = lax.axis_index("c")
    tp = lax.axis_index(PLANE)
    at = jnp.stack([z, c, tp]).astype(jnp.int32)
    ids = route_ids.T
    weights = route_weights.T

    local, qs, summary, own_residual, joined = pl.pallas_call(
        head_body,
        out_shape=[
            jax.ShapeDtypeStruct((R, W), F32),
            jax.ShapeDtypeStruct((2, R, W), F32),
            jax.ShapeDtypeStruct((2, W + 8, W), F32),
            jax.ShapeDtypeStruct((R, W), BF16),
            pltpu.HBM((6 * D, W), BF16),
        ],
        in_specs=[SMEM] + [HBM] * 10,
        out_specs=[VMEM] * 4 + [HBM],
        scratch_shapes=[pltpu.VMEM((6 * D, W), BF16)]
        + [pltpu.VMEM((R, W), BF16)] * 4
        + [pltpu.VMEM((1, R), F32), pltpu.VMEM((2, W), F32), pltpu.SemaphoreType.DMA((17,))],
        compiler_params=limit(8),
        name="head",
    )(
        at,
        *(
            in_hbm(x)
            for x in (
                query_in,
                value_in,
                forget_fwd,
                forget_bwd,
                jumps,
                gate_gap,
                residual,
                w_gate[0],
                w_up[0],
                w_down[0],
            )
        ),
    )
    plus = passed_on(joined, 1)
    minus = passed_on(joined, SIDE - 1)
    both = lax.all_gather(summary, "c")
    (packed,) = whole(pack_body, (((Z, W // 2 + 8, W), BF16),), [SMEM, VMEM])(at, both)
    packed = lax.all_to_all(packed, "z", 0, 0, tiled=True)
    (half,) = whole(carry_body, (((2, W // 2, W), F32),), [SMEM, VMEM])(at, packed)
    carry = lax.all_gather(half, "c")
    (terms,) = whole(mix_body, (((TP, R, W), BF16),), [SMEM] + [VMEM] * 7)(
        at, local, qs, both, carry, out_gate, head_gain.reshape(1, W), out_weight
    )
    terms = lax.all_to_all(terms, PLANE, 0, 0, tiled=True)

    stream, buffer = whole(
        send_body, (((R, W), BF16), ((Z, PAIR, W), BF16)), [SMEM] + [VMEM] * 3
    )(at, terms, own_residual, ids)

    buffer, plus, minus = lax.optimization_barrier((buffer, plus, minus))
    far0 = passed_on(plus[: 3 * D], 1)
    far1 = passed_on(minus[3 * D :], SIDE - 1)
    arrived = lax.all_to_all(buffer, "z", 0, 0, tiled=True)
    arrived = lax.all_gather(arrived, "c")
    (rows,) = whole(pick_body, (((SLOTS, W), BF16),), [SMEM, VMEM])(at, arrived)
    rows = exchange(rows.reshape(SIDE, PART, W), FIRST)
    rows, far0, far1 = lax.optimization_barrier((rows, far0, far1))
    rows = exchange(jnp.broadcast_to(rows, (SIDE, *rows.shape)), SECOND).reshape(TP, PART, W)

    active, down = pl.pallas_call(
        up_body,
        out_shape=[
            jax.ShapeDtypeStruct((SIDE, PART, SIDE * HID), BF16),
            pltpu.VMEM((2 * D, SIDE * W), BF16),
        ],
        in_specs=[SMEM, VMEM, VMEM] + [HBM] * 5,
        out_specs=[VMEM, IN_VMEM],
        scratch_shapes=[
            pltpu.VMEM((SIDE, 2, D, HID), BF16),
            pltpu.VMEM((PART, D), BF16),
            pltpu.SemaphoreType.DMA((5 * SIDE,)),
        ],
        compiler_params=limit(24),
        name="up",
    )(
        at,
        rows,
        norm_gain.reshape(1, D),
        *(in_hbm(w) for w in (joined, plus, minus, far0, far1)),
    )
    active = exchange(active, SECOND)
    (made,) = whole(down_body, (((SIDE, PART, W), BF16),), [SMEM, VMEM, VMEM])(at, active, down)
    produced = exchange(made, FIRST)

    back = lax.all_to_all(produced.reshape(Z, PAIR, W), "z", 0, 0, tiled=True)
    back = lax.all_gather(back, "c")
    (mixed,) = whole(return_body, (((R, W), BF16),), [SMEM] + [VMEM] * 4)(
        at, back, stream, ids, weights
    )
    return mixed


def solution(mesh):
    finer = Mesh(mesh.devices.reshape(Z, 2, SIDE, SIDE), ("z", "c", "y", "x"))
    return jax.shard_map(
        shards,
        mesh=finer,
        in_specs=(
            P(SP, None),
            P(SP, PLANE),
            P(SP, PLANE),
            P(SP, PLANE),
            P(SP, PLANE),
            P(PLANE, SP),
            P(None, PLANE),
            P(SP, PLANE),
            P(PLANE),
            P(PLANE, None),
            P(),
            P(SP, None),
            P(SP, None),
            P(SP, None, PLANE),
            P(SP, None, PLANE),
            P(SP, None, PLANE),
        ),
        out_specs=P(SP, PLANE),
        check_vma=False,
    )
```

```python
import jax
import jax.numpy as jnp
from jax import lax
from jax.experimental import pallas as pl
from jax.experimental.pallas import tpu as pltpu
from jax.sharding import Mesh
from jax.sharding import PartitionSpec as P

F32 = jnp.float32
BF16 = jnp.bfloat16
EPS = 1e-06
CAP = 36
PAIR = 2 * CAP
Z = 16
R = 192
W = 128
D = 2048
PART = 288
SIDE = 4
TP = SIDE * SIDE
HID = 256
SP = ("z", "c")
PLANE = ("y", "x")
CYX = ("c", "y", "x")


def place(c, y, x):
    return (c * SIDE + y) * SIDE + x


FOUR = range(SIDE)
FIRST = [[place(0, y, x) for x in FOUR] for y in FOUR] + [
    [place(1, y, x) for y in FOUR] for x in FOUR
]
SECOND = [[place(0, y, x) for y in FOUR] for x in FOUR] + [
    [place(1, y, x) for x in FOUR] for y in FOUR
]


def exchange(pieces, groups):
    return lax.all_to_all(pieces, CYX, 0, 0, axis_index_groups=groups, tiled=True)


def ring(step):
    return [
        (place(c, y, x), place(c, (y + step * c) % SIDE, (x + step * (1 - c)) % SIDE))
        for c in range(2)
        for y in FOUR
        for x in FOUR
    ]


def passed_on(x, step):
    return lax.ppermute(x, CYX, ring(step))


def dot(a, b, dims):
    return lax.dot_general(a, b, (dims, ((), ())), preferred_element_type=F32)


def split(a):
    high = a.astype(BF16)
    return high, (a - high.astype(F32)).astype(BF16)


def dot2(a, b, dims):
    high, low = split(a)
    return dot(high, b, dims) + dot(low, b, dims)


def dot3(a, b, dims):
    ah, al = split(a)
    bh, bl = split(b)
    return dot(ah, bh, dims) + (dot(ah, bl, dims) + dot(al, bh, dims))


def iota2(shape, dim):
    return lax.broadcasted_iota(jnp.int32, shape, dim)


def head_body(
    at_ref,
    q_hbm,
    v_hbm,
    ff_hbm,
    fb_hbm,
    jr_hbm,
    gap_hbm,
    res_hbm,
    wg_hbm,
    wu_hbm,
    wd_hbm,
    local_ref,
    qs_ref,
    sum_ref,
    res_ref,
    joined_hbm,
    held_ref,
    q_ref,
    v_ref,
    ff_ref,
    fb_ref,
    jr_ref,
    gap_ref,
    sems,
):
    own = pl.ds(pl.multiple_of(at_ref[2] * W, W), W)
    moves = (
        (q_hbm, q_ref),
        (ff_hbm, ff_ref),
        (jr_hbm, jr_ref),
        (gap_hbm, gap_ref),
        (v_hbm, v_ref),
        (fb_hbm, fb_ref),
        (res_hbm.at[:, own], res_ref),
    )
    copies = [pltpu.make_async_copy(a, b, sems.at[k]) for k, (a, b) in enumerate(moves)]
    inward = []
    outward = []
    for k, w_hbm in enumerate((wg_hbm, wg_hbm, wu_hbm, wu_hbm, wd_hbm)):
        rows = pl.ds(k * D, 2 * D if k == 4 else D)
        source = w_hbm if k == 4 else w_hbm.at[:, pl.ds((k % 2) * W, W)]
        held = held_ref.at[rows]
        inward.append(pltpu.make_async_copy(source, held, sems.at[7 + k]))
        outward.append(pltpu.make_async_copy(held, joined_hbm.at[rows], sems.at[12 + k]))
    for copy in copies + inward:
        copy.start()
    for copy in copies:
        copy.wait()
    q = q_ref[...].astype(F32)
    q = q * jax.nn.sigmoid(q)
    v = v_ref[...]
    row = iota2((R, R), 0)
    col = iota2((R, R), 1)
    jr = jr_ref[...]
    jc = jnp.sum(jnp.where(row == col, jr, 0.0), axis=1, keepdims=True)
    total = None
    for d, f_ref in enumerate((ff_ref, fb_ref)):
        if d == 1:
            for first, second in zip(inward, outward):
                first.wait()
                second.start()
        seen = (col <= row) if d == 0 else (col >= row)
        seen_t = (row <= col) if d == 0 else (row >= col)
        key = gap_ref[d : d + 1, :] * jax.nn.sigmoid(-f_ref[...].astype(F32))
        high, low = split(jnp.log1p(-key))
        ones = seen.astype(BF16)
        sums = dot(ones, high, ((1,), (0,))) + dot(ones, low, ((1,), (0,)))
        jump_c = jnp.sum(jnp.where(seen, jr, 0.0), axis=1, keepdims=True)
        jump_r = jnp.sum(jnp.where(seen_t, jc, 0.0), axis=0, keepdims=True)
        mid = sums[R // 2 : R // 2 + 1, :]
        scores = dot3(q * jnp.exp(sums - mid), key * jnp.exp(mid - sums), ((1,), (1,)))
        fade = jnp.exp(jnp.where(seen, jump_c - jump_r, -1e30))
        part = dot2(scores * fade, v, ((1,), (0,)))
        total = part if total is None else total + part
        last = R - 1 if d == 0 else 0
        end = sums[last : last + 1, :]
        end_jump = jump_c[last : last + 1, :]
        key_end = key * jnp.exp((end - sums) + (end_jump - jump_c))
        high, low = split(key_end)
        sum_ref[d, 0:W, :] = dot(v, high, ((0,), (0,))) + dot(v, low, ((0,), (0,)))
        sum_ref[d, W : W + 8, :] = jnp.broadcast_to(jnp.exp(end + end_jump), (8, W))
        qs_ref[d] = q * jnp.exp(sums + jump_c)
    local_ref[...] = total
    for copy in outward:
        copy.wait()


def pack_body(at_ref, sum_ref, out_ref):
    z = at_ref[0]
    c = at_ref[1]
    start = pl.multiple_of(c * (W // 2), W // 2)

    def message(d):
        near, far = (1, 0) if d == 0 else (0, 1)
        near_decay = sum_ref[near, d, W : W + 1, :]
        decay = sum_ref[far, d, W : W + 1, :] * near_decay
        state = (
            sum_ref[far, d, pl.ds(start, W // 2), :] * near_decay
            + sum_ref[near, d, pl.ds(start, W // 2), :]
        )
        high = decay.astype(BF16).astype(F32)
        low = decay - high
        line = iota2((8, W), 0)
        tail = jnp.where(line == 0, high, jnp.where(line == 1, low, 0.0))
        return jnp.concatenate([state, tail], axis=0).astype(BF16)

    fwd = message(0)
    bwd = message(1)
    for k in range(Z):
        later = jnp.full((W // 2 + 8, W), k, jnp.int32) > z
        out_ref[k] = jnp.where(later, fwd.astype(F32), bwd.astype(F32)).astype(BF16)


def carry_body(at_ref, got_ref, out_ref):
    z = at_ref[0]

    def step(k, carry):
        got = got_ref[k].astype(F32)
        return carry * (got[W // 2 : W // 2 + 1] + got[W // 2 + 1 : W // 2 + 2]) + got[: W // 2]

    zero = jnp.zeros((W // 2, W), F32)
    out_ref[0] = lax.fori_loop(0, z, step, zero)
    out_ref[1] = lax.fori_loop(0, Z - 1 - z, lambda k, s: step(Z - 1 - k, s), zero)


def mix_body(at_ref, local_ref, qs_ref, sum_ref, carry_ref, gate_ref, gain_ref, w_ref, out_ref):
    c = at_ref[1]
    o = local_ref[...]
    for d in range(2):
        carry = jnp.concatenate([carry_ref[0, d], carry_ref[1, d]], axis=0)
        through = carry * sum_ref[d, d, W : W + 1, :] + sum_ref[d, d, 0:W, :]
        passed = jnp.full((W, W), c, jnp.int32) != d
        o = o + dot3(qs_ref[d], jnp.where(passed, through, carry), ((1,), (1,)))
    mean_square = jnp.mean(o * o, axis=1, keepdims=True)
    gate = gate_ref[...].astype(F32)
    gated = o * lax.rsqrt(mean_square + EPS) * gain_ref[...] * (gate * jax.nn.sigmoid(gate))
    terms = dot(gated.astype(BF16), w_ref[...], ((1,), (0,))).astype(BF16)
    for k in range(TP):
        out_ref[k] = terms[:, k * W : (k + 1) * W]


def slots_of(ids, expert):
    named = ids[0:1] == expert
    for j in range(1, 4):
        named = named | (ids[j : j + 1] == expert)
    before = (iota2((R, R), 0) < iota2((R, R), 1)).astype(BF16)
    rank = dot(named.astype(BF16), before, ((1,), (0,)))
    return jnp.where(named, rank, -1000.0)


def send_body(at_ref, got_ref, res_ref, ids_ref, stream_ref, out_ref):
    total = got_ref[0].astype(F32)
    for k in range(1, TP):
        total = total + got_ref[k].astype(F32)
    stream = (res_ref[...].astype(F32) + total).astype(BF16)
    stream_ref[...] = stream
    slots = slots_of(ids_ref[...], iota2((32, R), 0))
    line = iota2((PAIR, R), 0).astype(F32)
    for z in range(Z):
        hit = (line == slots[2 * z : 2 * z + 1]) | (line == slots[2 * z + 1 : 2 * z + 2] + CAP)
        out_ref[z] = dot(hit.astype(BF16), stream, ((1,), (0,))).astype(BF16)


def pick_body(at_ref, got_ref, out_ref):
    c = at_ref[1]
    line = iota2((PAIR, 2 * PAIR), 0)
    source = iota2((PAIR, 2 * PAIR), 1)
    wanted = line + c * CAP + jnp.where(line < CAP, 0, PAIR - CAP)
    choose = (source == wanted).astype(BF16)
    for z in range(Z):
        both = jnp.concatenate([got_ref[0, z], got_ref[1, z]], axis=0)
        rows = dot(choose, both, ((1,), (0,))).astype(BF16)
        a, place_in = divmod(z, SIDE)
        for b in range(SIDE):
            target = jnp.where(c == 0, b * SIDE + a, a * SIDE + b)
            out_ref[target, place_in * PAIR : (place_in + 1) * PAIR, :] = rows


def up_body(
    x_ref, gain_ref, wg, wu, wd, plus, minus, far0, far1, out_ref, wd_ref, w_ref, rows_ref, sems
):
    def piece(q, k, rows):
        start = k * D
        if q == 0:
            return wd if k == 4 else (wg, wu)[k // 2].at[:, pl.ds((k % 2) * W, W)]
        if q < 3:
            return (plus, minus)[q - 1].at[pl.ds(start, rows)]
        return (far0, far1)[start // (3 * D)].at[pl.ds(start % (3 * D), rows)]

    copies = []
    for q in range(SIDE):
        for k in range(4):
            target = w_ref.at[q, k // 2, :, pl.ds((k % 2) * W, W)]
            copies.append(pltpu.make_async_copy(piece(q, k, D), target, sems.at[5 * q + k]))
    for q in range(SIDE):
        target = wd_ref.at[:, pl.ds(q * W, W)]
        copies.append(pltpu.make_async_copy(piece(q, 4, 2 * D), target, sems.at[5 * q + 4]))
    for copy in copies:
        copy.start()
    squares = None
    for p in range(TP):
        x = x_ref[p].astype(F32)
        squares = x * x if squares is None else squares + x * x
    scale = lax.rsqrt(jnp.sum(squares, axis=1, keepdims=True) / D + EPS)
    for p in range(TP):
        cols = pl.ds(p * W, W)
        rows_ref[:, cols] = (x_ref[p].astype(F32) * scale * gain_ref[:, cols]).astype(BF16)
    rows = rows_ref[...]
    for q in range(SIDE):
        for copy in copies[4 * q : 4 * q + 4]:
            copy.wait()
        c = jnp.minimum(dot(rows, w_ref[q, 0], ((1,), (0,))), 7.0)
        u = jnp.clip(dot(rows, w_ref[q, 1], ((1,), (0,))), -7.0, 7.0)
        active = (c * jax.nn.sigmoid(1.702 * c) * (u + 1.0)).astype(BF16)
        for k in range(SIDE):
            out_ref[k, :, q * HID : (q + 1) * HID] = active
    for copy in copies[4 * SIDE :]:
        copy.wait()


def along(at_ref, q):
    a = jnp.where(at_ref[1] == 0, at_ref[2] % SIDE, at_ref[2] // SIDE)
    return (a + (0, SIDE - 1, 1, 2)[q]) % SIDE


def down_body(at_ref, act_ref, w_ref, out_ref):
    made = None
    for q in range(SIDE):
        a = along(at_ref, q)
        for b in range(SIDE):
            share = jnp.where(at_ref[1] == 0, b * SIDE + a, a * SIDE + b)
            w = w_ref[pl.ds(pl.multiple_of(share * HID, HID), HID), :]
            term = dot(act_ref[b, :, q * HID : (q + 1) * HID], w, ((1,), (0,)))
            made = term if made is None else made + term
    made = made.astype(BF16)
    for q in range(SIDE):
        out_ref[along(at_ref, q)] = made[:, q * W : (q + 1) * W]


def halves_body(plus_hbm, minus_hbm, first_hbm, second_hbm, held_ref, sems):
    half = 3 * D
    parts = ((plus_hbm.at[pl.ds(0, half)], first_hbm), (minus_hbm.at[pl.ds(half, half)], second_hbm))
    inward = []
    outward = []
    for k, (source, target) in enumerate(parts):
        inward.append(pltpu.make_async_copy(source, held_ref.at[k], sems.at[k]))
        outward.append(pltpu.make_async_copy(held_ref.at[k], target, sems.at[2 + k]))
    for copy in inward:
        copy.start()
    for first, second in zip(inward, outward):
        first.wait()
        second.start()
    for copy in outward:
        copy.wait()


def shares_body(at_ref, ids_ref, weights_ref, high_ref, low_ref):
    ids = ids_ref[...]
    weights = weights_ref[...]
    group = iota2((32, R), 0)
    expert = jnp.where(group < Z, 2 * group, 2 * group - 31)
    slots = slots_of(ids, expert)
    share = jnp.where(ids[0:1] == expert, weights[0:1], 0.0)
    for j in range(1, 4):
        share = share + jnp.where(ids[j : j + 1] == expert, weights[j : j + 1], 0.0)
    line = iota2((32, 32 * PAIR), 1)
    first = iota2((32, 32 * PAIR), 0) * PAIR
    inside = (line >= first) & (line < first + PAIR)
    spread = inside.astype(BF16)
    place_in = jnp.sum(jnp.where(inside, line - first, 0), axis=0, keepdims=True)
    rank = (place_in - at_ref[1] * CAP).astype(F32)
    high, low = split(share)
    slot_at = dot(slots.astype(BF16), spread, ((0,), (0,)))
    hit = slot_at == rank
    high_ref[...] = jnp.where(hit, dot(high, spread, ((0,), (0,))), 0.0).astype(BF16)
    low_ref[...] = jnp.where(hit, dot(low, spread, ((0,), (0,))), 0.0).astype(BF16)


def return_body(got_ref, stream_ref, high_ref, low_ref, out_ref):
    got = jnp.concatenate([got_ref[k, z] for k in range(2) for z in range(Z)], axis=0)
    total = dot(high_ref[...], got, ((1,), (0,))) + dot(low_ref[...], got, ((1,), (0,)))
    out_ref[...] = (stream_ref[...].astype(F32) + total).astype(BF16)


def limit(mib):
    return pltpu.CompilerParams(vmem_limit_bytes=mib << 20)


VMEM = pl.BlockSpec()
SMEM = pl.BlockSpec(memory_space=pltpu.SMEM)
HBM = pl.BlockSpec(memory_space=pltpu.HBM)
IN_VMEM = pl.BlockSpec(memory_space=pltpu.VMEM)


def in_hbm(x):
    return pltpu.with_memory_space_constraint(x, pltpu.HBM)


def whole(body, outs, specs, room=12):
    return pl.pallas_call(
        body,
        out_shape=[jax.ShapeDtypeStruct(s, t) for s, t in outs],
        in_specs=specs,
        out_specs=[VMEM] * len(outs),
        compiler_params=limit(room),
    )


def shards(
    residual,
    query_in,
    value_in,
    forget_fwd,
    forget_bwd,
    jumps,
    gate_gap,
    out_gate,
    head_gain,
    out_weight,
    norm_gain,
    route_ids,
    route_weights,
    w_gate,
    w_up,
    w_down,
):
    z = lax.axis_index("z")
    c = lax.axis_index("c")
    tp = lax.axis_index(PLANE)
    at = jnp.stack([z, c, tp]).astype(jnp.int32)
    ids = route_ids.T
    weights = route_weights.T

    local, qs, summary, own_residual, joined = pl.pallas_call(
        head_body,
        out_shape=[
            jax.ShapeDtypeStruct((R, W), F32),
            jax.ShapeDtypeStruct((2, R, W), F32),
            jax.ShapeDtypeStruct((2, W + 8, W), F32),
            jax.ShapeDtypeStruct((R, W), BF16),
            pltpu.HBM((6 * D, W), BF16),
        ],
        in_specs=[SMEM] + [HBM] * 10,
        out_specs=[VMEM] * 4 + [HBM],
        scratch_shapes=[pltpu.VMEM((6 * D, W), BF16)]
        + [pltpu.VMEM((R, W), BF16)] * 4
        + [pltpu.VMEM((1, R), F32), pltpu.VMEM((2, W), F32), pltpu.SemaphoreType.DMA((17,))],
        compiler_params=limit(8),
        name="head",
    )(
        at,
        *(
            in_hbm(x)
            for x in (
                query_in,
                value_in,
                forget_fwd,
                forget_bwd,
                jumps,
                gate_gap,
                residual,
                w_gate[0],
                w_up[0],
                w_down[0],
            )
        ),
    )
    plus = passed_on(joined, 1)
    minus = passed_on(joined, SIDE - 1)
    both = lax.all_gather(summary, "c")
    (packed,) = whole(pack_body, (((Z, W // 2 + 8, W), BF16),), [SMEM, VMEM])(at, both)
    packed = lax.all_to_all(packed, "z", 0, 0, tiled=True)
    (half,) = whole(carry_body, (((2, W // 2, W), F32),), [SMEM, VMEM])(at, packed)
    carry = lax.all_gather(half, "c")
    (terms,) = whole(mix_body, (((TP, R, W), BF16),), [SMEM] + [VMEM] * 7)(
        at, local, qs, both, carry, out_gate, head_gain.reshape(1, W), out_weight
    )
    terms = lax.all_to_all(terms, PLANE, 0, 0, tiled=True)

    stream, buffer = whole(
        send_body, (((R, W), BF16), ((Z, PAIR, W), BF16)), [SMEM] + [VMEM] * 3
    )(at, terms, own_residual, ids)

    buffer, plus, minus = lax.optimization_barrier((buffer, plus, minus))
    first_half, second_half = pl.pallas_call(
        halves_body,
        out_shape=[pltpu.HBM((3 * D, W), BF16)] * 2,
        in_specs=[HBM, HBM],
        out_specs=[HBM, HBM],
        scratch_shapes=[pltpu.VMEM((2, 3 * D, W), BF16), pltpu.SemaphoreType.DMA((4,))],
        compiler_params=limit(8),
        name="halves",
    )(in_hbm(plus), in_hbm(minus))
    far0 = passed_on(first_half, 1)
    far1 = passed_on(second_half, SIDE - 1)
    arrived = lax.all_to_all(buffer, "z", 0, 0, tiled=True)
    high, low = pl.pallas_call(
        shares_body,
        out_shape=[pltpu.VMEM((R, 32 * PAIR), BF16)] * 2,
        in_specs=[SMEM, VMEM, VMEM],
        out_specs=[IN_VMEM, IN_VMEM],
        compiler_params=limit(12),
        name="shares",
    )(at, ids, weights)
    arrived = lax.all_gather(arrived, "c")
    (rows,) = whole(pick_body, (((TP, PART, W), BF16),), [SMEM, VMEM])(at, arrived)
    rows = lax.all_to_all(rows, PLANE, 0, 0, tiled=True)

    active, down = pl.pallas_call(
        up_body,
        out_shape=[
            jax.ShapeDtypeStruct((SIDE, PART, SIDE * HID), BF16),
            pltpu.VMEM((2 * D, SIDE * W), BF16),
        ],
        in_specs=[VMEM, VMEM] + [HBM] * 7,
        out_specs=[VMEM, IN_VMEM],
        scratch_shapes=[
            pltpu.VMEM((SIDE, 2, D, HID), BF16),
            pltpu.VMEM((PART, D), BF16),
            pltpu.SemaphoreType.DMA((5 * SIDE,)),
        ],
        compiler_params=limit(24),
        name="up",
    )(
        rows,
        norm_gain.reshape(1, D),
        *(in_hbm(w) for w in (w_gate[0], w_up[0], w_down[0], plus, minus, far0, far1)),
    )
    active = exchange(active, SECOND)
    (made,) = whole(down_body, (((SIDE, PART, W), BF16),), [SMEM, VMEM, VMEM])(at, active, down)
    produced = exchange(made, FIRST)

    back = lax.all_to_all(produced.reshape(Z, PAIR, W), "z", 0, 0, tiled=True)
    back = lax.all_gather(back, "c")
    (mixed,) = whole(return_body, (((R, W), BF16),), [VMEM, VMEM, IN_VMEM, IN_VMEM])(
        back, stream, high, low
    )
    return mixed


def solution(mesh):
    finer = Mesh(mesh.devices.reshape(Z, 2, SIDE, SIDE), ("z", "c", "y", "x"))
    return jax.shard_map(
        shards,
        mesh=finer,
        in_specs=(
            P(SP, None),
            P(SP, PLANE),
            P(SP, PLANE),
            P(SP, PLANE),
            P(SP, PLANE),
            P(PLANE, SP),
            P(None, PLANE),
            P(SP, PLANE),
            P(PLANE),
            P(PLANE, None),
            P(),
            P(SP, None),
            P(SP, None),
            P(SP, None, PLANE),
            P(SP, None, PLANE),
            P(SP, None, PLANE),
        ),
        out_specs=P(SP, PLANE),
        check_vma=False,
    )
```

```python
import jax
import jax.numpy as jnp
from jax import lax
from jax.experimental import pallas as pl
from jax.experimental.pallas import tpu as pltpu
from jax.sharding import Mesh
from jax.sharding import PartitionSpec as P

F32 = jnp.float32
BF16 = jnp.bfloat16
EPS = 1e-06
CAP = 36
PAIR = 2 * CAP
Z = 16
R = 192
W = 128
D = 2048
PART = 288
SIDE = 4
TP = SIDE * SIDE
HID = 256
SP = ("z", "c")
PLANE = ("y", "x")
CYX = ("c", "y", "x")


def place(c, y, x):
    return (c * SIDE + y) * SIDE + x


FOUR = range(SIDE)
FIRST = [[place(0, y, x) for x in FOUR] for y in FOUR] + [
    [place(1, y, x) for y in FOUR] for x in FOUR
]
SECOND = [[place(0, y, x) for y in FOUR] for x in FOUR] + [
    [place(1, y, x) for x in FOUR] for y in FOUR
]


def exchange(pieces, groups):
    return lax.all_to_all(pieces, CYX, 0, 0, axis_index_groups=groups, tiled=True)


def ring(step):
    return [
        (place(c, y, x), place(c, (y + step * c) % SIDE, (x + step * (1 - c)) % SIDE))
        for c in range(2)
        for y in FOUR
        for x in FOUR
    ]


def passed_on(x, step):
    return lax.ppermute(x, CYX, ring(step))


def dot(a, b, dims):
    return lax.dot_general(a, b, (dims, ((), ())), preferred_element_type=F32)


def split(a):
    high = a.astype(BF16)
    return high, (a - high.astype(F32)).astype(BF16)


def dot2(a, b, dims):
    high, low = split(a)
    return dot(high, b, dims) + dot(low, b, dims)


def dot3(a, b, dims):
    ah, al = split(a)
    bh, bl = split(b)
    return dot(ah, bh, dims) + (dot(ah, bl, dims) + dot(al, bh, dims))


def iota2(shape, dim):
    return lax.broadcasted_iota(jnp.int32, shape, dim)


def head_body(
    at_ref,
    q_hbm,
    v_hbm,
    ff_hbm,
    fb_hbm,
    jr_hbm,
    gap_hbm,
    res_hbm,
    wg_hbm,
    wu_hbm,
    wd_hbm,
    local_ref,
    qs_ref,
    sum_ref,
    res_ref,
    joined_hbm,
    held_ref,
    q_ref,
    v_ref,
    ff_ref,
    fb_ref,
    jr_ref,
    gap_ref,
    sems,
):
    own = pl.ds(pl.multiple_of(at_ref[2] * W, W), W)
    moves = (
        (q_hbm, q_ref),
        (ff_hbm, ff_ref),
        (jr_hbm, jr_ref),
        (gap_hbm, gap_ref),
        (v_hbm, v_ref),
        (fb_hbm, fb_ref),
        (res_hbm.at[:, own], res_ref),
    )
    copies = [pltpu.make_async_copy(a, b, sems.at[k]) for k, (a, b) in enumerate(moves)]
    inward = []
    outward = []
    for k, w_hbm in enumerate((wg_hbm, wg_hbm, wu_hbm, wu_hbm, wd_hbm)):
        rows = pl.ds(k * D, 2 * D if k == 4 else D)
        source = w_hbm if k == 4 else w_hbm.at[:, pl.ds((k % 2) * W, W)]
        held = held_ref.at[rows]
        inward.append(pltpu.make_async_copy(source, held, sems.at[7 + k]))
        outward.append(pltpu.make_async_copy(held, joined_hbm.at[rows], sems.at[12 + k]))
    for copy in copies + inward:
        copy.start()
    for copy in copies:
        copy.wait()
    q = q_ref[...].astype(F32)
    q = q * jax.nn.sigmoid(q)
    v = v_ref[...]
    row = iota2((R, R), 0)
    col = iota2((R, R), 1)
    jr = jr_ref[...]
    jc = jnp.sum(jnp.where(row == col, jr, 0.0), axis=1, keepdims=True)
    total = None
    for d, f_ref in enumerate((ff_ref, fb_ref)):
        if d == 1:
            for first, second in zip(inward, outward):
                first.wait()
                second.start()
        seen = (col <= row) if d == 0 else (col >= row)
        seen_t = (row <= col) if d == 0 else (row >= col)
        key = gap_ref[d : d + 1, :] * jax.nn.sigmoid(-f_ref[...].astype(F32))
        high, low = split(jnp.log1p(-key))
        ones = seen.astype(BF16)
        sums = dot(ones, high, ((1,), (0,))) + dot(ones, low, ((1,), (0,)))
        jump_c = jnp.sum(jnp.where(seen, jr, 0.0), axis=1, keepdims=True)
        jump_r = jnp.sum(jnp.where(seen_t, jc, 0.0), axis=0, keepdims=True)
        mid = sums[R // 2 : R // 2 + 1, :]
        scores = dot3(q * jnp.exp(sums - mid), key * jnp.exp(mid - sums), ((1,), (1,)))
        fade = jnp.exp(jnp.where(seen, jump_c - jump_r, -1e30))
        part = dot2(scores * fade, v, ((1,), (0,)))
        total = part if total is None else total + part
        last = R - 1 if d == 0 else 0
        end = sums[last : last + 1, :]
        end_jump = jump_c[last : last + 1, :]
        key_end = key * jnp.exp((end - sums) + (end_jump - jump_c))
        high, low = split(key_end)
        sum_ref[d, 0:W, :] = dot(v, high, ((0,), (0,))) + dot(v, low, ((0,), (0,)))
        sum_ref[d, W : W + 8, :] = jnp.broadcast_to(jnp.exp(end + end_jump), (8, W))
        qs_ref[d] = q * jnp.exp(sums + jump_c)
    local_ref[...] = total
    for copy in outward:
        copy.wait()


def pack_body(at_ref, sum_ref, out_ref):
    z = at_ref[0]
    c = at_ref[1]
    start = pl.multiple_of(c * (W // 2), W // 2)

    def message(d):
        near, far = (1, 0) if d == 0 else (0, 1)
        near_decay = sum_ref[near, d, W : W + 1, :]
        decay = sum_ref[far, d, W : W + 1, :] * near_decay
        state = (
            sum_ref[far, d, pl.ds(start, W // 2), :] * near_decay
            + sum_ref[near, d, pl.ds(start, W // 2), :]
        )
        high = decay.astype(BF16).astype(F32)
        low = decay - high
        line = iota2((8, W), 0)
        tail = jnp.where(line == 0, high, jnp.where(line == 1, low, 0.0))
        return jnp.concatenate([state, tail], axis=0).astype(BF16)

    fwd = message(0)
    bwd = message(1)
    for k in range(Z):
        later = jnp.full((W // 2 + 8, W), k, jnp.int32) > z
        out_ref[k] = jnp.where(later, fwd.astype(F32), bwd.astype(F32)).astype(BF16)


def carry_body(at_ref, got_ref, out_ref):
    z = at_ref[0]

    def step(k, carry):
        got = got_ref[k].astype(F32)
        return carry * (got[W // 2 : W // 2 + 1] + got[W // 2 + 1 : W // 2 + 2]) + got[: W // 2]

    zero = jnp.zeros((W // 2, W), F32)
    out_ref[0] = lax.fori_loop(0, z, step, zero)
    out_ref[1] = lax.fori_loop(0, Z - 1 - z, lambda k, s: step(Z - 1 - k, s), zero)


def mix_body(at_ref, local_ref, qs_ref, sum_ref, carry_ref, gate_ref, gain_ref, w_ref, out_ref):
    c = at_ref[1]
    o = local_ref[...]
    for d in range(2):
        carry = jnp.concatenate([carry_ref[0, d], carry_ref[1, d]], axis=0)
        through = carry * sum_ref[d, d, W : W + 1, :] + sum_ref[d, d, 0:W, :]
        passed = jnp.full((W, W), c, jnp.int32) != d
        o = o + dot3(qs_ref[d], jnp.where(passed, through, carry), ((1,), (1,)))
    mean_square = jnp.mean(o * o, axis=1, keepdims=True)
    gate = gate_ref[...].astype(F32)
    gated = o * lax.rsqrt(mean_square + EPS) * gain_ref[...] * (gate * jax.nn.sigmoid(gate))
    terms = dot(gated.astype(BF16), w_ref[...], ((1,), (0,))).astype(BF16)
    for k in range(TP):
        out_ref[k] = terms[:, k * W : (k + 1) * W]


def slots_of(ids, expert):
    named = ids[0:1] == expert
    for j in range(1, 4):
        named = named | (ids[j : j + 1] == expert)
    before = (iota2((R, R), 0) < iota2((R, R), 1)).astype(BF16)
    rank = dot(named.astype(BF16), before, ((1,), (0,)))
    return jnp.where(named, rank, -1000.0)


def send_body(got_ref, res_ref, ids_ref, stream_ref, out_hbm, held_ref, sems):
    total = got_ref[0].astype(F32)
    for k in range(1, TP):
        total = total + got_ref[k].astype(F32)
    stream = (res_ref[...].astype(F32) + total).astype(BF16)
    stream_ref[...] = stream
    slots = slots_of(ids_ref[...], iota2((32, R), 0))
    line = iota2((PAIR, R), 0).astype(F32)
    copies = []
    for z in range(Z):
        hit = (line == slots[2 * z : 2 * z + 1]) | (line == slots[2 * z + 1 : 2 * z + 2] + CAP)
        held_ref[z] = dot(hit.astype(BF16), stream, ((1,), (0,))).astype(BF16)
        copies.append(pltpu.make_async_copy(held_ref.at[z], out_hbm.at[z], sems.at[z]))
        copies[z].start()
    for copy in copies:
        copy.wait()


def pick_body(at_ref, got_ref, out_hbm, held_ref, sems):
    c = at_ref[1]
    line = iota2((PAIR, 2 * PAIR), 0)
    source = iota2((PAIR, 2 * PAIR), 1)
    wanted = line + c * CAP + jnp.where(line < CAP, 0, PAIR - CAP)
    choose = (source == wanted).astype(BF16)
    copies = []
    for a in range(SIDE):
        for part in range(SIDE):
            z = a * SIDE + part
            both = jnp.concatenate([got_ref[0, z], got_ref[1, z]], axis=0)
            rows = dot(choose, both, ((1,), (0,))).astype(BF16)
            held_ref[a, part * PAIR : (part + 1) * PAIR, :] = rows
        for b in range(SIDE):
            target = jnp.where(c == 0, b * SIDE + a, a * SIDE + b)
            k = a * SIDE + b
            copies.append(pltpu.make_async_copy(held_ref.at[a], out_hbm.at[target], sems.at[k]))
            copies[k].start()
    for copy in copies:
        copy.wait()


def up_body(
    x_ref, gain_ref, wg, wu, wd, plus, minus, far0, far1, out_ref, wd_ref, w_ref, rows_ref, sems
):
    def piece(q, k, rows):
        start = k * D
        if q == 0:
            return wd if k == 4 else (wg, wu)[k // 2].at[:, pl.ds((k % 2) * W, W)]
        if q < 3:
            return (plus, minus)[q - 1].at[pl.ds(start, rows)]
        return (far0, far1)[start // (3 * D)].at[pl.ds(start % (3 * D), rows)]

    copies = []
    for q in range(SIDE):
        for k in range(4):
            target = w_ref.at[q, k // 2, :, pl.ds((k % 2) * W, W)]
            copies.append(pltpu.make_async_copy(piece(q, k, D), target, sems.at[5 * q + k]))
    for q in range(SIDE):
        target = wd_ref.at[:, pl.ds(q * W, W)]
        copies.append(pltpu.make_async_copy(piece(q, 4, 2 * D), target, sems.at[5 * q + 4]))
    for copy in copies:
        copy.start()
    squares = None
    for p in range(TP):
        x = x_ref[p].astype(F32)
        squares = x * x if squares is None else squares + x * x
    scale = lax.rsqrt(jnp.sum(squares, axis=1, keepdims=True) / D + EPS)
    for p in range(TP):
        cols = pl.ds(p * W, W)
        rows_ref[:, cols] = (x_ref[p].astype(F32) * scale * gain_ref[:, cols]).astype(BF16)
    rows = rows_ref[...]
    for q in range(SIDE):
        for copy in copies[4 * q : 4 * q + 4]:
            copy.wait()
        c = jnp.minimum(dot(rows, w_ref[q, 0], ((1,), (0,))), 7.0)
        u = jnp.clip(dot(rows, w_ref[q, 1], ((1,), (0,))), -7.0, 7.0)
        active = (c * jax.nn.sigmoid(1.702 * c) * (u + 1.0)).astype(BF16)
        for k in range(SIDE):
            out_ref[k, :, q * HID : (q + 1) * HID] = active
    for copy in copies[4 * SIDE :]:
        copy.wait()


def along(at_ref, q):
    a = jnp.where(at_ref[1] == 0, at_ref[2] % SIDE, at_ref[2] // SIDE)
    return (a + (0, SIDE - 1, 1, 2)[q]) % SIDE


def down_body(at_ref, act_ref, w_ref, out_ref):
    made = None
    for q in range(SIDE):
        a = along(at_ref, q)
        for b in range(SIDE):
            share = jnp.where(at_ref[1] == 0, b * SIDE + a, a * SIDE + b)
            w = w_ref[pl.ds(pl.multiple_of(share * HID, HID), HID), :]
            term = dot(act_ref[b, :, q * HID : (q + 1) * HID], w, ((1,), (0,)))
            made = term if made is None else made + term
    made = made.astype(BF16)
    for q in range(SIDE):
        out_ref[along(at_ref, q)] = made[:, q * W : (q + 1) * W]


def halves_body(plus_hbm, minus_hbm, first_hbm, second_hbm, held_ref, sems):
    half = 3 * D
    parts = ((plus_hbm.at[pl.ds(0, half)], first_hbm), (minus_hbm.at[pl.ds(half, half)], second_hbm))
    inward = []
    outward = []
    for k, (source, target) in enumerate(parts):
        inward.append(pltpu.make_async_copy(source, held_ref.at[k], sems.at[k]))
        outward.append(pltpu.make_async_copy(held_ref.at[k], target, sems.at[2 + k]))
    for copy in inward:
        copy.start()
    for first, second in zip(inward, outward):
        first.wait()
        second.start()
    for copy in outward:
        copy.wait()


def shares_body(at_ref, ids_ref, weights_ref, high_ref, low_ref):
    ids = ids_ref[...]
    weights = weights_ref[...]
    group = iota2((32, R), 0)
    expert = jnp.where(group < Z, 2 * group, 2 * group - 31)
    slots = slots_of(ids, expert)
    share = jnp.where(ids[0:1] == expert, weights[0:1], 0.0)
    for j in range(1, 4):
        share = share + jnp.where(ids[j : j + 1] == expert, weights[j : j + 1], 0.0)
    line = iota2((32, 32 * PAIR), 1)
    first = iota2((32, 32 * PAIR), 0) * PAIR
    inside = (line >= first) & (line < first + PAIR)
    spread = inside.astype(BF16)
    place_in = jnp.sum(jnp.where(inside, line - first, 0), axis=0, keepdims=True)
    rank = (place_in - at_ref[1] * CAP).astype(F32)
    high, low = split(share)
    slot_at = dot(slots.astype(BF16), spread, ((0,), (0,)))
    hit = slot_at == rank
    high_ref[...] = jnp.where(hit, dot(high, spread, ((0,), (0,))), 0.0).astype(BF16)
    low_ref[...] = jnp.where(hit, dot(low, spread, ((0,), (0,))), 0.0).astype(BF16)


def return_body(got_ref, stream_ref, high_ref, low_ref, out_ref):
    got = jnp.concatenate([got_ref[k, z] for k in range(2) for z in range(Z)], axis=0)
    total = dot(high_ref[...], got, ((1,), (0,))) + dot(low_ref[...], got, ((1,), (0,)))
    out_ref[...] = (stream_ref[...].astype(F32) + total).astype(BF16)


def limit(mib):
    return pltpu.CompilerParams(vmem_limit_bytes=mib << 20)


VMEM = pl.BlockSpec()
SMEM = pl.BlockSpec(memory_space=pltpu.SMEM)
HBM = pl.BlockSpec(memory_space=pltpu.HBM)
IN_VMEM = pl.BlockSpec(memory_space=pltpu.VMEM)


def in_hbm(x):
    return pltpu.with_memory_space_constraint(x, pltpu.HBM)


def whole(body, outs, specs, room=12):
    return pl.pallas_call(
        body,
        out_shape=[jax.ShapeDtypeStruct(s, t) for s, t in outs],
        in_specs=specs,
        out_specs=[VMEM] * len(outs),
        compiler_params=limit(room),
    )


def shards(
    residual,
    query_in,
    value_in,
    forget_fwd,
    forget_bwd,
    jumps,
    gate_gap,
    out_gate,
    head_gain,
    out_weight,
    norm_gain,
    route_ids,
    route_weights,
    w_gate,
    w_up,
    w_down,
):
    z = lax.axis_index("z")
    c = lax.axis_index("c")
    tp = lax.axis_index(PLANE)
    at = jnp.stack([z, c, tp]).astype(jnp.int32)
    ids = route_ids.T
    weights = route_weights.T

    local, qs, summary, own_residual, joined = pl.pallas_call(
        head_body,
        out_shape=[
            jax.ShapeDtypeStruct((R, W), F32),
            jax.ShapeDtypeStruct((2, R, W), F32),
            jax.ShapeDtypeStruct((2, W + 8, W), F32),
            jax.ShapeDtypeStruct((R, W), BF16),
            pltpu.HBM((6 * D, W), BF16),
        ],
        in_specs=[SMEM] + [HBM] * 10,
        out_specs=[VMEM] * 4 + [HBM],
        scratch_shapes=[pltpu.VMEM((6 * D, W), BF16)]
        + [pltpu.VMEM((R, W), BF16)] * 4
        + [pltpu.VMEM((1, R), F32), pltpu.VMEM((2, W), F32), pltpu.SemaphoreType.DMA((17,))],
        compiler_params=limit(8),
        name="head",
    )(
        at,
        *(
            in_hbm(x)
            for x in (
                query_in,
                value_in,
                forget_fwd,
                forget_bwd,
                jumps,
                gate_gap,
                residual,
                w_gate[0],
                w_up[0],
                w_down[0],
            )
        ),
    )
    plus = passed_on(joined, 1)
    minus = passed_on(joined, SIDE - 1)
    both = lax.all_gather(summary, "c")
    (packed,) = whole(pack_body, (((Z, W // 2 + 8, W), BF16),), [SMEM, VMEM])(at, both)
    packed = lax.all_to_all(packed, "z", 0, 0, tiled=True)
    (half,) = whole(carry_body, (((2, W // 2, W), F32),), [SMEM, VMEM])(at, packed)
    carry = lax.all_gather(half, "c")
    (terms,) = whole(mix_body, (((TP, R, W), BF16),), [SMEM] + [VMEM] * 7)(
        at, local, qs, both, carry, out_gate, head_gain.reshape(1, W), out_weight
    )
    terms = lax.all_to_all(terms, PLANE, 0, 0, tiled=True)

    stream, buffer = pl.pallas_call(
        send_body,
        out_shape=[jax.ShapeDtypeStruct((R, W), BF16), pltpu.HBM((Z, PAIR, W), BF16)],
        in_specs=[VMEM] * 3,
        out_specs=[VMEM, HBM],
        scratch_shapes=[pltpu.VMEM((Z, PAIR, W), BF16), pltpu.SemaphoreType.DMA((Z,))],
        compiler_params=limit(12),
        name="send",
    )(terms, own_residual, ids)

    buffer, plus, minus = lax.optimization_barrier((buffer, plus, minus))
    first_half, second_half = pl.pallas_call(
        halves_body,
        out_shape=[pltpu.HBM((3 * D, W), BF16)] * 2,
        in_specs=[HBM, HBM],
        out_specs=[HBM, HBM],
        scratch_shapes=[pltpu.VMEM((2, 3 * D, W), BF16), pltpu.SemaphoreType.DMA((4,))],
        compiler_params=limit(8),
        name="halves",
    )(in_hbm(plus), in_hbm(minus))
    far0 = passed_on(first_half, 1)
    far1 = passed_on(second_half, SIDE - 1)
    arrived = lax.all_to_all(buffer, "z", 0, 0, tiled=True)
    arrived = lax.all_gather(arrived, "c")
    rows = pl.pallas_call(
        pick_body,
        out_shape=pltpu.HBM((TP, PART, W), BF16),
        in_specs=[SMEM, VMEM],
        out_specs=HBM,
        scratch_shapes=[pltpu.VMEM((SIDE, PART, W), BF16), pltpu.SemaphoreType.DMA((TP,))],
        compiler_params=limit(12),
        name="pick",
    )(at, arrived)
    rows = lax.all_to_all(rows, PLANE, 0, 0, tiled=True)
    high, low = pl.pallas_call(
        shares_body,
        out_shape=[pltpu.VMEM((R, 32 * PAIR), BF16)] * 2,
        in_specs=[SMEM, VMEM, VMEM],
        out_specs=[IN_VMEM, IN_VMEM],
        compiler_params=limit(12),
        name="shares",
    )(at, ids, weights)

    active, down = pl.pallas_call(
        up_body,
        out_shape=[
            jax.ShapeDtypeStruct((SIDE, PART, SIDE * HID), BF16),
            pltpu.VMEM((2 * D, SIDE * W), BF16),
        ],
        in_specs=[VMEM, VMEM] + [HBM] * 7,
        out_specs=[VMEM, IN_VMEM],
        scratch_shapes=[
            pltpu.VMEM((SIDE, 2, D, HID), BF16),
            pltpu.VMEM((PART, D), BF16),
            pltpu.SemaphoreType.DMA((5 * SIDE,)),
        ],
        compiler_params=limit(24),
        name="up",
    )(
        rows,
        norm_gain.reshape(1, D),
        *(in_hbm(w) for w in (w_gate[0], w_up[0], w_down[0], plus, minus, far0, far1)),
    )
    active = exchange(active, SECOND)
    (made,) = whole(down_body, (((SIDE, PART, W), BF16),), [SMEM, VMEM, VMEM])(at, active, down)
    produced = exchange(made, FIRST)

    back = lax.all_to_all(produced.reshape(Z, PAIR, W), "z", 0, 0, tiled=True)
    back = lax.all_gather(back, "c")
    (mixed,) = whole(return_body, (((R, W), BF16),), [VMEM, VMEM, IN_VMEM, IN_VMEM])(
        back, stream, high, low
    )
    return mixed


def solution(mesh):
    finer = Mesh(mesh.devices.reshape(Z, 2, SIDE, SIDE), ("z", "c", "y", "x"))
    return jax.shard_map(
        shards,
        mesh=finer,
        in_specs=(
            P(SP, None),
            P(SP, PLANE),
            P(SP, PLANE),
            P(SP, PLANE),
            P(SP, PLANE),
            P(PLANE, SP),
            P(None, PLANE),
            P(SP, PLANE),
            P(PLANE),
            P(PLANE, None),
            P(),
            P(SP, None),
            P(SP, None),
            P(SP, None, PLANE),
            P(SP, None, PLANE),
            P(SP, None, PLANE),
        ),
        out_specs=P(SP, PLANE),
        check_vma=False,
    )
```
